32 devices in a mesh: dp: 4 (over y, x), kv: 4 (over z), tp: 2 (over core).
Axes of the slice: x: 2, y: 2, z: 4, core: 2. Of those that a mesh axis runs over, the one named last changes fastest.
Arguments:
- stream: bfloat16 [32, 2048], P('dp', ('kv', 'tp')), parts along dimension 0, may hold values from -40 to 40
- old_state: float32 [32, 8, 64, 128], P(('dp', 'kv'), 'tp'), parts along dimension 0, may hold values from -6 to 6
- decay_amounts: float32 [32, 512], P(('dp', 'kv'), 'tp'), parts along dimension 0, may hold values from 0.003 to 1
- first_gain: float32 [2048], replicated, may hold values from 0.1 to 1.9
- first_gate: bfloat16 [2048, 5632], P(None, ('kv', 'tp')), may hold values from -0.125 to 0.125
- first_up: bfloat16 [2048, 5632], P(None, ('kv', 'tp')), may hold values from -0.125 to 0.125
- first_down: bfloat16 [5632, 2048], P(('kv', 'tp')), may hold values from -0.078125 to 0.078125
- mixer_gain: float32 [2048], P('kv'), may hold values from 0.1 to 1.9
- query_weight: bfloat16 [2048, 512], P('kv', 'tp'), may hold values from -0.125 to 0.125
- key_weight: bfloat16 [2048, 512], P('kv', 'tp'), may hold values from -0.125 to 0.125
- decay_weight: bfloat16 [2048, 512], P('kv', 'tp'), may hold values from -0.5 to 0.5
- value_weight: bfloat16 [2048, 1024], P('kv', 'tp'), may hold values from -0.125 to 0.125
- output_gate_weight: bfloat16 [2048, 1024], P('kv', 'tp'), may hold values from -0.125 to 0.125
- head_gain: float32 [1024], P('tp'), may hold values from 0.1 to 1.9
- output_weight: bfloat16 [1024, 2048], P('tp', 'kv'), may hold values from -0.1875 to 0.1875
- second_gain: float32 [2048], replicated, may hold values from 0.1 to 1.9
- second_gate: bfloat16 [2048, 5632], P(None, ('kv', 'tp')), may hold values from -0.125 to 0.125
- second_up: bfloat16 [2048, 5632], P(None, ('kv', 'tp')), may hold values from -0.125 to 0.125
- second_down: bfloat16 [5632, 2048], P(('kv', 'tp')), may hold values from -0.078125 to 0.078125
Outputs:
- mixed_stream: bfloat16 [32, 2048], P('dp', ('kv', 'tp')), parts along dimension 0
- new_state: float32 [32, 8, 64, 128], P(('dp', 'kv'), 'tp'), parts along dimension 0
The draws below stay inside these ranges and needn't reach their ends.
There are 4 independent parts, one for each index of `dp`. The reference program is written for one: setup_inputs(seed, part) draws one part's arguments, and reference() takes and returns one part's arrays. A program takes and returns all parts, laid end to end along the dimension named above; an argument that names none is the same for every part. Nothing has to cross between parts.
All inputs are finite; a program needn't handle non-finite values.
Results may differ from the reference program's by a relative error of at most 0.007.
Values may be sent and summed in bfloat16 or wider, within the bound.
A program may use at most 64 MiB of HBM per device.

```python
import math
import jax
import jax.numpy as jnp
from jax import lax

D = 2048
FF = 5632
HEAD_TOTAL = 8
KEY_CHANNELS = 64
VALUE_DIM = 128
SEQS = 8
N_TP = 2


def draw_stream(key, part):
    first_key = jax.random.fold_in(key, 11)
    second_key = jax.random.fold_in(key, 12)
    columns = jnp.arange(D, dtype=jnp.float32)
    rising = 1.0 + 2.0 * columns / D
    rough = jnp.exp(jax.random.uniform(second_key, (D,), jnp.float32, -0.4, 0.4))
    base = jnp.clip(jax.random.normal(first_key, (SEQS, D), jnp.float32), -4.0, 4.0)
    return (base * rising * rough).astype(jnp.bfloat16)


def block_levels(stream_key, shape, cuts, smallest, largest):
    gain = 1.0
    for position, parts in cuts:
        steps = jax.random.uniform(jax.random.fold_in(jax.random.fold_in(stream_key, 6), position), (parts,), jnp.float32, smallest / len(cuts), largest / len(cuts))
        gain = gain * jnp.repeat(jnp.exp(steps), shape[position] // parts).reshape((-1,) + (1,) * (len(shape) - 1 - position))
    return gain


def bell_draw(stream_key, extent, scale, limit, cuts=(), kind=jnp.bfloat16):
    level = block_levels(stream_key, extent, cuts, -0.22, 0.18) if cuts else 1.0
    array = jax.random.normal(stream_key, extent, jnp.float32) * scale * level
    return jnp.minimum(jnp.maximum(array, -limit), limit).astype(kind)


def setup_inputs(seed: int = 0, part: int = 0) -> dict:
    arg_keys = jax.random.split(jax.random.key(seed), 20)
    part_keys = jax.random.split(jax.random.fold_in(arg_keys[19], part), 20)
    stream = draw_stream(jax.random.fold_in(jax.random.fold_in(arg_keys[19], part), 71), part)
    old_state = bell_draw(part_keys[1], (SEQS, HEAD_TOTAL, KEY_CHANNELS, VALUE_DIM), 1.0, 6.0, ((0, 4), (1, 2)), jnp.float32)
    decay_amounts = jnp.clip(jnp.exp(math.log(1.0) - 5.809143 * jax.random.uniform(part_keys[2], (SEQS, HEAD_TOTAL * KEY_CHANNELS), jnp.float32) ** block_levels(part_keys[2], (SEQS, HEAD_TOTAL * KEY_CHANNELS), ((0, 4), (1, 2)), -0.2, 0.2)), 0.003, 1.0)
    first_gain = jnp.clip(1.0 + 0.18 * jax.random.normal(arg_keys[3], (D,), jnp.float32), 0.1, 1.9)
    first_gate = bell_draw(arg_keys[4], (D, FF), D ** -0.5, 0.125, ((1, 8),))
    first_up = bell_draw(arg_keys[5], (D, FF), D ** -0.5, 0.125, ((1, 8),))
    first_down = bell_draw(arg_keys[6], (FF, D), FF ** -0.5, 0.078125, ((0, 8),))
    mixer_gain = jnp.clip(1.0 + 0.18 * jax.random.normal(arg_keys[7], (D,), jnp.float32), 0.1, 1.9)
    query_weight = bell_draw(arg_keys[8], (D, HEAD_TOTAL * KEY_CHANNELS), D ** -0.5, 0.125, ((0, 4), (1, 2)))
    key_weight = bell_draw(arg_keys[9], (D, HEAD_TOTAL * KEY_CHANNELS), D ** -0.5, 0.125, ((0, 4), (1, 2)))
    decay_weight = bell_draw(arg_keys[10], (D, HEAD_TOTAL * KEY_CHANNELS), (D // 16) ** -0.5, 0.5, ((0, 4), (1, 2)))
    value_weight = bell_draw(arg_keys[11], (D, HEAD_TOTAL * VALUE_DIM), D ** -0.5, 0.125, ((0, 4), (1, 2)))
    output_gate_weight = bell_draw(arg_keys[12], (D, HEAD_TOTAL * VALUE_DIM), D ** -0.5, 0.125, ((0, 4), (1, 2)))
    head_gain = jnp.clip(1.0 + 0.18 * jax.random.normal(arg_keys[13], (HEAD_TOTAL * VALUE_DIM,), jnp.float32), 0.1, 1.9)
    output_weight = bell_draw(arg_keys[14], (HEAD_TOTAL * VALUE_DIM, D), (HEAD_TOTAL * VALUE_DIM) ** -0.5, 0.1875, ((0, 2), (1, 4)))
    second_gain = jnp.clip(1.0 + 0.18 * jax.random.normal(arg_keys[15], (D,), jnp.float32), 0.1, 1.9)
    second_gate = bell_draw(arg_keys[16], (D, FF), D ** -0.5, 0.125, ((1, 8),))
    second_up = bell_draw(arg_keys[17], (D, FF), D ** -0.5, 0.125, ((1, 8),))
    second_down = bell_draw(arg_keys[18], (FF, D), FF ** -0.5, 0.078125, ((0, 8),))
    return {"stream": stream, "old_state": old_state, "decay_amounts": decay_amounts, "first_gain": first_gain, "first_gate": first_gate, "first_up": first_up, "first_down": first_down, "mixer_gain": mixer_gain, "query_weight": query_weight, "key_weight": key_weight, "decay_weight": decay_weight, "value_weight": value_weight, "output_gate_weight": output_gate_weight, "head_gain": head_gain, "output_weight": output_weight, "second_gain": second_gain, "second_gate": second_gate, "second_up": second_up, "second_down": second_down}


EPSILON = 1e-06
GATE_SOFTNESS = 16.0

def row_scale_of(rows):
    wide = rows.astype(jnp.float32)
    return lax.rsqrt(lax.optimization_barrier(jnp.mean(wide * wide, axis=-1, keepdims=True)) + EPSILON)

def half_block(stream, norm_gain, w_gate, w_up, w_down):
    row_scale = row_scale_of(stream)
    scaled = (stream.astype(jnp.float32) * norm_gain).astype(jnp.bfloat16)
    gate_part = jnp.dot(scaled, w_gate, preferred_element_type=jnp.float32) * row_scale
    up_part = jnp.dot(scaled, w_up, preferred_element_type=jnp.float32) * row_scale
    hidden = (jax.nn.silu(gate_part) * up_part).astype(jnp.bfloat16)
    result = stream.astype(jnp.float32) + 0.5 * jnp.dot(hidden, w_down, preferred_element_type=jnp.float32)
    return result.astype(jnp.bfloat16)

def reference(stream, old_state, decay_amounts, first_gain, first_gate, first_up, first_down, mixer_gain, query_weight, key_weight, decay_weight, value_weight, output_gate_weight, head_gain, output_weight, second_gain, second_gate, second_up, second_down):
    middle = half_block(stream, first_gain, first_gate, first_up, first_down)
    row_scale = row_scale_of(middle)
    scaled = (middle.astype(jnp.float32) * mixer_gain).astype(jnp.bfloat16)

    def project(weight_block):
        return jnp.dot(scaled, weight_block, preferred_element_type=jnp.float32) * row_scale
    sequence_count = stream.shape[0]
    query = (project(query_weight) * KEY_CHANNELS ** (-0.5)).reshape(sequence_count, HEAD_TOTAL, KEY_CHANNELS)
    keys = project(key_weight).reshape(sequence_count, HEAD_TOTAL, KEY_CHANNELS)
    gate_logits = project(decay_weight).reshape(sequence_count, HEAD_TOTAL, KEY_CHANNELS)
    values = project(value_weight).reshape(sequence_count, HEAD_TOTAL, VALUE_DIM)
    out_gate = project(output_gate_weight)
    decay_logarithm = jax.nn.log_sigmoid(gate_logits) / GATE_SOFTNESS - decay_amounts.reshape(sequence_count, HEAD_TOTAL, KEY_CHANNELS)
    new_state = jnp.exp(decay_logarithm)[..., None] * old_state + keys[..., None] * values[:, :, None, :]
    readout = jnp.einsum('bhk,bhkv->bhv', query, new_state, precision=lax.Precision.HIGHEST)
    normed = readout * lax.rsqrt(lax.optimization_barrier(jnp.mean(readout * readout, axis=-1, keepdims=True)) + EPSILON)
    mixed_heads = (normed.reshape(sequence_count, HEAD_TOTAL * VALUE_DIM) * head_gain * jax.nn.silu(out_gate)).astype(jnp.bfloat16)
    group_width = HEAD_TOTAL * VALUE_DIM // N_TP
    attention_out = jnp.zeros((sequence_count, D), jnp.float32)
    for group in range(N_TP):
        partial_out = jnp.dot(mixed_heads[:, group * group_width:(group + 1) * group_width], output_weight[group * group_width:(group + 1) * group_width], preferred_element_type=jnp.float32).astype(jnp.bfloat16)
        attention_out = attention_out + lax.optimization_barrier(partial_out).astype(jnp.float32)
    after = (middle.astype(jnp.float32) + attention_out).astype(jnp.bfloat16)
    mixed_stream = half_block(after, second_gain, second_gate, second_up, second_down)
    return (mixed_stream, new_state)
```

```python
import functools

import jax
import jax.numpy as jnp
from jax import lax
from jax.experimental import pallas as pl
from jax.experimental.pallas import tpu as pltpu
from jax.sharding import PartitionSpec as P

EPSILON = 1e-06
GATE_SOFTNESS = 16.0
MESH = pl.DeviceIdType.MESH
F32 = jnp.float32
BF16 = jnp.bfloat16


def dot(a, b):
    return jnp.dot(a, b, preferred_element_type=F32)


def layer_kernel(
    n_kv,
    n_tp,
    stream_h,
    state_h,
    amounts_h,
    gain1_h,
    gate1_h,
    up1_h,
    down1_h,
    mixgain_h,
    query_h,
    key_h,
    decay_h,
    value_h,
    outgate_h,
    headgain_h,
    output_h,
    gain2_h,
    gate2_h,
    up2_h,
    down2_h,
    out_ref,
    newstate_h,
    stream_v,
    state_v,
    amounts_v,
    gain1_v,
    gate1_v,
    up1_v,
    down1_v,
    mixgain_v,
    proj_v,
    headgain_v,
    output_v,
    gain2_v,
    gate2_v,
    up2_v,
    down2_v,
    newstate_v,
    wide_v,
    down_out,
    down_in,
    middle_v,
    proj_out,
    proj_in,
    mixed_v,
    attn_v,
    after_v,
    last_out,
    last_in,
    load_sem,
    store_sem,
    a_send,
    a_recv,
    c_send,
    c_recv,
    d_send,
    d_recv,
    m_send,
    m_recv,
    e_send,
    e_recv,
    g_send,
    g_recv,
    h_send,
    h_recv,
):
    z = lax.axis_index("kv")
    c = lax.axis_index("tp")
    me = z * n_tp + c
    seqs, own_cols = stream_v.shape
    chip_cols = own_cols * n_tp
    width = chip_cols * n_kv
    rows, heads, key_dim, value_dim = state_v.shape
    key_cols = heads * key_dim
    value_cols = heads * value_dim

    loads = []

    def load(src, dst):
        copy = pltpu.make_async_copy(src, dst, load_sem.at[len(loads)])
        copy.start()
        loads.append(copy)
        return copy

    load_stream = load(stream_h, stream_v)
    load_gain1 = load(gain1_h, gain1_v)
    load_gate1 = load(gate1_h, gate1_v)
    load_up1 = load(up1_h, up1_v)
    load_down1 = load(down1_h, down1_v)

    far = []
    for j in range(n_kv - 1):
        down_t = n_kv - 1 - j
        low = jnp.where(down_t <= z, down_t - 1, down_t)
        high = jnp.where(j >= z, j + 1, j)
        far.append(jnp.where(z < n_kv // 2, low, high))
    cores = [lax.rem(c + k, n_tp) for k in range(n_tp)]
    peers = [(t, k) for t in far for k in cores] + [(z, k) for k in cores[1:]]

    barrier = pltpu.get_barrier_semaphore()
    for t, k in peers:
        pl.semaphore_signal(barrier, inc=1, device_id={"kv": t, "tp": k}, device_id_type=MESH)
    pl.semaphore_wait(barrier, len(peers))

    sent = []

    def send(src, dst, send_sem, recv_sem, t, k):
        copy = pltpu.make_async_remote_copy(
            src_ref=src,
            dst_ref=dst,
            send_sem=send_sem,
            recv_sem=recv_sem,
            device_id={"kv": t, "tp": k},
            device_id_type=MESH,
        )
        copy.start()
        sent.append(copy)

    def arrived(ref, send_sem, recv_sem, t, k):
        pltpu.make_async_remote_copy(
            src_ref=ref,
            dst_ref=ref,
            send_sem=send_sem,
            recv_sem=recv_sem,
            device_id={"kv": t, "tp": k},
            device_id_type=MESH,
        ).wait_recv()

    load_stream.wait()
    for p, (t, k) in enumerate(peers):
        send(stream_v, wide_v.at[me], a_send.at[p], a_recv.at[me], t, k)
    wide_v[me] = stream_v[...]

    load_state = load(state_h, state_v)
    load_small = [load(amounts_h, amounts_v), load(headgain_h, headgain_v)]
    load_mix = [load(mixgain_h, mixgain_v)]
    at = 0
    for ref in (query_h, key_h, decay_h, value_h, outgate_h):
        load_mix.append(load(ref, proj_v.at[:, at : at + ref.shape[1]]))
        at += ref.shape[1]
    proj_cols = at
    load_output = load(output_h, output_v)
    load_second = [load(gain2_h, gain2_v), load(gate2_h, gate2_v), load(up2_h, up2_v)]
    load_down2 = load(down2_h, down2_v)

    load_gain1.wait()
    load_gate1.wait()
    load_up1.wait()
    gate_acc = jnp.zeros((seqs, gate1_v.shape[1]), F32)
    up_acc = jnp.zeros((seqs, up1_v.shape[1]), F32)
    squares = jnp.zeros((seqs, 1), F32)
    order = [(z, k) for k in cores] + [(t, k) for t in far[::-1] for k in cores]
    for i, (t, k) in enumerate(order):
        who = t * n_tp + k
        if i:
            arrived(wide_v.at[who], a_send.at[0], a_recv.at[who], t, k)
        block = wide_v[who].astype(F32)
        cols = pl.ds(pl.multiple_of(who * own_cols, own_cols), own_cols)
        scaled = (block * gain1_v[:, cols]).astype(BF16)
        squares += jnp.sum(block * block, axis=1, keepdims=True)
        gate_acc += dot(scaled, gate1_v[cols, :])
        up_acc += dot(scaled, up1_v[cols, :])
    scale = lax.rsqrt(squares / width + EPSILON)
    hidden = (jax.nn.silu(gate_acc * scale) * (up_acc * scale)).astype(BF16)

    load_down1.wait()
    for j, t in enumerate(far):
        cols = pl.ds(pl.multiple_of(t * chip_cols, chip_cols), chip_cols)
        down_out[j] = dot(hidden, down1_v[:, cols]).astype(BF16)
        for i, k in enumerate(cores):
            send(down_out.at[j], down_in.at[me], c_send.at[j * n_tp + i], c_recv.at[me], t, k)
    cols = pl.ds(pl.multiple_of(z * chip_cols, chip_cols), chip_cols)
    own = dot(hidden, down1_v[:, cols])
    down_out[n_kv - 1] = own.astype(BF16)
    for i, k in enumerate(cores[1:]):
        send(
            down_out.at[n_kv - 1],
            down_in.at[me],
            c_send.at[(n_kv - 1) * n_tp + i],
            c_recv.at[me],
            z,
            k,
        )
    summed = own.astype(BF16).astype(F32)
    for t, k in order[1:]:
        who = t * n_tp + k
        arrived(down_in.at[who], c_send.at[0], c_recv.at[who], t, k)
        summed += down_in[who].astype(F32)
    chip_stream = jnp.concatenate([wide_v[z * n_tp + i] for i in range(n_tp)], axis=1)
    middle = (chip_stream.astype(F32) + 0.5 * summed).astype(BF16)
    middle_v[z] = middle

    for copy in load_mix:
        copy.wait()
    middle_wide = middle.astype(F32)
    scaled = (middle_wide * mixgain_v[...]).astype(BF16)
    part = dot(scaled, proj_v[...])
    square_part = jnp.broadcast_to(
        jnp.sum(middle_wide * middle_wide, axis=1, keepdims=True), (seqs, 128)
    )
    for j in range(n_kv):
        proj_out[j, :, :proj_cols] = part[j * rows : (j + 1) * rows]
        proj_out[j, :, proj_cols:] = square_part[j * rows : (j + 1) * rows]
    for j, t in enumerate(far):
        send(proj_out.at[t], proj_in.at[z], d_send.at[j], d_recv.at[z], t, c)
    for j, t in enumerate(far):
        send(middle_v.at[z], middle_v.at[z], m_send.at[j], m_recv.at[z], t, c)

    total = proj_out[z]
    for t in far[::-1]:
        arrived(proj_in.at[t], d_send.at[0], d_recv.at[t], t, c)
        total += proj_in[t]
    scale = lax.rsqrt(total[:, proj_cols : proj_cols + 1] / width + EPSILON)
    total = total[:, :proj_cols] * scale
    query = total[:, :key_cols] * key_dim ** (-0.5)
    keys = total[:, key_cols : 2 * key_cols]
    logits = total[:, 2 * key_cols : 3 * key_cols]
    values = total[:, 3 * key_cols : 3 * key_cols + value_cols]
    outgate = total[:, 3 * key_cols + value_cols :]
    for copy in load_small:
        copy.wait()
    log_sigmoid = jnp.minimum(logits, 0.0) - jnp.log(1.0 + jnp.exp(-jnp.abs(logits)))
    decay = jnp.exp(log_sigmoid / GATE_SOFTNESS - amounts_v[...])
    stacked = jnp.concatenate(
        [query, keys, decay, jnp.zeros((128 - 3 * rows, key_cols), F32)], axis=0
    )
    turned = stacked.T
    gated = headgain_v[...] * jax.nn.silu(outgate)
    load_state.wait()
    mixed_rows = []
    for b in range(rows):
        pieces = []
        for h in range(heads):
            span = slice(h * key_dim, (h + 1) * key_dim)
            lane = slice(h * value_dim, (h + 1) * value_dim)
            q_col = turned[span, b : b + 1]
            k_col = turned[span, rows + b : rows + b + 1]
            d_col = turned[span, 2 * rows + b : 2 * rows + b + 1]
            new = d_col * state_v[b, h] + k_col * values[b : b + 1, lane]
            newstate_v[b, h] = new
            readout = jnp.sum(q_col * new, axis=0, keepdims=True)
            normed = readout * lax.rsqrt(
                jnp.mean(readout * readout, axis=1, keepdims=True) + EPSILON
            )
            pieces.append(normed * gated[b : b + 1, lane])
        mixed_rows.append(jnp.concatenate(pieces, axis=1))
    store = pltpu.make_async_copy(newstate_v, newstate_h, store_sem)

    mixed_v[z] = jnp.concatenate(mixed_rows, axis=0).astype(BF16).astype(F32)
    for j, t in enumerate(far):
        send(mixed_v.at[z], mixed_v.at[z], e_send.at[j], e_recv.at[z], t, c)
    store.start()
    load_output.wait()
    for t in far[::-1]:
        arrived(mixed_v.at[t], e_send.at[0], e_recv.at[t], t, c)
    mixed = jnp.concatenate([mixed_v[j] for j in range(n_kv)], axis=0).astype(BF16)
    attn_v[me] = dot(mixed, output_v[...]).astype(BF16)

    for p, (t, k) in enumerate(peers):
        send(attn_v.at[me], attn_v.at[me], g_send.at[p], g_recv.at[me], t, k)
    for copy in load_second:
        copy.wait()
    gate_acc = jnp.zeros((seqs, gate2_v.shape[1]), F32)
    up_acc = jnp.zeros((seqs, up2_v.shape[1]), F32)
    squares = jnp.zeros((seqs, 1), F32)
    for t in [z] + far[::-1]:
        if t is not z:
            arrived(middle_v.at[t], m_send.at[0], m_recv.at[t], t, c)
        attention = jnp.zeros((seqs, chip_cols), F32)
        for k in cores:
            who = t * n_tp + k
            if not (t is z and k is cores[0]):
                arrived(attn_v.at[who], g_send.at[0], g_recv.at[who], t, k)
            attention += attn_v[who].astype(F32)
        after = (middle_v[t].astype(F32) + attention).astype(BF16)
        block = after.astype(F32)
        if t is z:
            for i in range(n_tp):
                after_v[i] = block[:, i * own_cols : (i + 1) * own_cols]
        cols = pl.ds(pl.multiple_of(t * chip_cols, chip_cols), chip_cols)
        scaled = (block * gain2_v[:, cols]).astype(BF16)
        squares += jnp.sum(block * block, axis=1, keepdims=True)
        gate_acc += dot(scaled, gate2_v[cols, :])
        up_acc += dot(scaled, up2_v[cols, :])
    scale = lax.rsqrt(squares / width + EPSILON)
    hidden = (jax.nn.silu(gate_acc * scale) * (up_acc * scale)).astype(BF16)

    load_down2.wait()
    for j, t in enumerate(far):
        cols = pl.ds(pl.multiple_of(t * chip_cols, chip_cols), chip_cols)
        piece = dot(hidden, down2_v[:, cols]).astype(BF16)
        for k in range(n_tp):
            last_out[j, k] = piece[:, k * own_cols : (k + 1) * own_cols]
            send(last_out.at[j, k], last_in.at[me], h_send.at[j * n_tp + k], h_recv.at[me], t, k)
    cols = pl.ds(pl.multiple_of(z * chip_cols, chip_cols), chip_cols)
    piece = dot(hidden, down2_v[:, cols]).astype(BF16)
    for k in range(n_tp):
        last_out[n_kv - 1, k] = piece[:, k * own_cols : (k + 1) * own_cols]
    for i, k in enumerate(cores[1:]):
        send(
            last_out.at[n_kv - 1, k],
            last_in.at[me],
            h_send.at[(n_kv - 1) * n_tp + i],
            h_recv.at[me],
            z,
            k,
        )
    summed = last_out[n_kv - 1, c].astype(F32)
    for t, k in order[1:]:
        who = t * n_tp + k
        arrived(last_in.at[who], h_send.at[0], h_recv.at[who], t, k)
        summed += last_in[who].astype(F32)
    out_ref[...] = (after_v[c] + 0.5 * summed).astype(BF16)

    store.wait()
    for copy in sent:
        copy.wait_send()


def half_block(stream, norm_gain, w_gate, w_up, w_down):
    wide = lax.all_gather(stream, ("kv", "tp"), axis=1, tiled=True).astype(jnp.float32)
    scaled = (wide * norm_gain).astype(jnp.bfloat16)
    gate_acc = jnp.dot(scaled, w_gate, preferred_element_type=jnp.float32)
    up_acc = jnp.dot(scaled, w_up, preferred_element_type=jnp.float32)
    square_acc = jnp.sum(wide * wide, axis=1)
    row_scale = lax.rsqrt(square_acc / norm_gain.shape[0] + EPSILON)[:, None]
    hidden = (jax.nn.silu(gate_acc * row_scale) * (up_acc * row_scale)).astype(jnp.bfloat16)
    partial_out = jnp.dot(hidden, w_down, preferred_element_type=jnp.float32)
    summed = lax.psum_scatter(partial_out, ("kv", "tp"), scatter_dimension=1, tiled=True)
    return (stream.astype(jnp.float32) + 0.5 * summed).astype(jnp.bfloat16)


def portable_body(
    stream,
    old_state,
    decay_amounts,
    first_gain,
    first_gate,
    first_up,
    first_down,
    mixer_gain,
    query_weight,
    key_weight,
    decay_weight,
    value_weight,
    output_gate_weight,
    head_gain,
    output_weight,
    second_gain,
    second_gate,
    second_up,
    second_down,
):
    middle = half_block(stream, first_gain, first_gate, first_up, first_down)
    paired_cols = lax.all_gather(middle, "tp", axis=1, tiled=True)
    wide_cols = paired_cols.astype(jnp.float32)
    scaled = (wide_cols * mixer_gain).astype(jnp.bfloat16)
    query_part = jnp.dot(scaled, query_weight, preferred_element_type=jnp.float32)
    key_part = jnp.dot(scaled, key_weight, preferred_element_type=jnp.float32)
    decay_part = jnp.dot(scaled, decay_weight, preferred_element_type=jnp.float32)
    value_part = jnp.dot(scaled, value_weight, preferred_element_type=jnp.float32)
    outgate_part = jnp.dot(scaled, output_gate_weight, preferred_element_type=jnp.float32)
    local_rows = old_state.shape[0]
    local_heads = old_state.shape[1]
    key_dim = old_state.shape[2]
    value_dim = old_state.shape[3]
    query_sum, key_sum, decay_sum, value_sum, outgate_sum, own_squares = (
        lax.psum_scatter(query_part, "kv", scatter_dimension=0, tiled=True),
        lax.psum_scatter(key_part, "kv", scatter_dimension=0, tiled=True),
        lax.psum_scatter(decay_part, "kv", scatter_dimension=0, tiled=True),
        lax.psum_scatter(value_part, "kv", scatter_dimension=0, tiled=True),
        lax.psum_scatter(outgate_part, "kv", scatter_dimension=0, tiled=True),
        lax.psum_scatter(
            jnp.sum(wide_cols * wide_cols, axis=1), "kv", scatter_dimension=0, tiled=True
        ),
    )
    row_scale = lax.rsqrt(own_squares / first_gain.shape[0] + EPSILON)[:, None]
    query = (query_sum * row_scale * key_dim ** (-0.5)).reshape(local_rows, local_heads, key_dim)
    keys = (key_sum * row_scale).reshape(local_rows, local_heads, key_dim)
    gate_logits = (decay_sum * row_scale).reshape(local_rows, local_heads, key_dim)
    values = (value_sum * row_scale).reshape(local_rows, local_heads, value_dim)
    decay_logarithm = jax.nn.log_sigmoid(gate_logits) / GATE_SOFTNESS - decay_amounts.reshape(
        local_rows, local_heads, key_dim
    )
    new_state = (
        jnp.exp(decay_logarithm)[..., None] * old_state + keys[..., None] * values[:, :, None, :]
    )
    readout = jnp.einsum("bhk,bhkv->bhv", query, new_state, precision=lax.Precision.HIGHEST)
    normed = readout * lax.rsqrt(jnp.mean(readout * readout, axis=-1, keepdims=True) + EPSILON)
    mixed_heads = (
        normed.reshape(local_rows, local_heads * value_dim)
        * head_gain
        * jax.nn.silu(outgate_sum * row_scale)
    ).astype(jnp.bfloat16)
    projected = jnp.dot(
        lax.all_gather(mixed_heads, "kv", axis=0, tiled=True),
        output_weight,
        preferred_element_type=jnp.float32,
    ).astype(jnp.bfloat16)
    attention_out = lax.psum_scatter(
        lax.optimization_barrier(projected).astype(jnp.float32).astype(jnp.bfloat16),
        "tp",
        scatter_dimension=1,
        tiled=True,
    ).astype(jnp.float32)
    after = (middle.astype(jnp.float32) + attention_out).astype(jnp.bfloat16)
    mixed_stream = half_block(after, second_gain, second_gate, second_up, second_down)
    return (mixed_stream, new_state)


def body(n_kv, n_tp, *args):
    (
        stream,
        old_state,
        decay_amounts,
        first_gain,
        first_gate,
        first_up,
        first_down,
        mixer_gain,
        query_weight,
        key_weight,
        decay_weight,
        value_weight,
        output_gate_weight,
        head_gain,
        output_weight,
        second_gain,
        second_gate,
        second_up,
        second_down,
    ) = args
    seqs, own_cols = stream.shape
    chip_cols = own_cols * n_tp
    rows, heads, key_dim, value_dim = old_state.shape
    if own_cols % 128 or value_dim % 128 or 3 * rows > 128 or n_kv * n_tp > 16:
        return portable_body(*args)
    proj_cols = 3 * heads * key_dim + 2 * heads * value_dim
    n = n_kv * n_tp
    first_gain, mixer_gain, head_gain, second_gain = (
        g.reshape(1, -1) for g in (first_gain, mixer_gain, head_gain, second_gain)
    )

    def like(array):
        return pltpu.VMEM(array.shape, array.dtype)

    dma = pltpu.SemaphoreType.DMA
    scratch = [
        like(stream),
        like(old_state),
        like(decay_amounts),
        like(first_gain),
        like(first_gate),
        like(first_up),
        like(first_down),
        like(mixer_gain),
        pltpu.VMEM((chip_cols, proj_cols), BF16),
        like(head_gain),
        like(output_weight),
        like(second_gain),
        like(second_gate),
        like(second_up),
        like(second_down),
        like(old_state),
        pltpu.VMEM((n, seqs, own_cols), BF16),
        pltpu.VMEM((n_kv, seqs, chip_cols), BF16),
        pltpu.VMEM((n, seqs, chip_cols), BF16),
        pltpu.VMEM((n_kv, seqs, chip_cols), BF16),
        pltpu.VMEM((n_kv, rows, proj_cols + 128), F32),
        pltpu.VMEM((n_kv, rows, proj_cols + 128), F32),
        pltpu.VMEM((n_kv, rows, heads * value_dim), F32),
        pltpu.VMEM((n, seqs, chip_cols), BF16),
        pltpu.VMEM((n_tp, seqs, own_cols), F32),
        pltpu.VMEM((n_kv, n_tp, seqs, own_cols), BF16),
        pltpu.VMEM((n, seqs, own_cols), BF16),
        dma((19,)),
        dma,
        dma((n,)),
        dma((n,)),
        dma((n,)),
        dma((n,)),
        dma((n_kv,)),
        dma((n_kv,)),
        dma((n_kv,)),
        dma((n_kv,)),
        dma((n_kv,)),
        dma((n_kv,)),
        dma((n,)),
        dma((n,)),
        dma((n,)),
        dma((n,)),
    ]
    return pl.pallas_call(
        functools.partial(layer_kernel, n_kv, n_tp),
        out_shape=(
            jax.ShapeDtypeStruct(stream.shape, stream.dtype),
            jax.ShapeDtypeStruct(old_state.shape, old_state.dtype),
        ),
        in_specs=[pl.BlockSpec(memory_space=pl.ANY)] * 19,
        out_specs=(
            pl.BlockSpec(memory_space=pltpu.VMEM),
            pl.BlockSpec(memory_space=pl.ANY),
        ),
        scratch_shapes=scratch,
        compiler_params=pltpu.CompilerParams(
            collective_id=0, has_side_effects=True, vmem_limit_bytes=60 * 1024 * 1024
        ),
        name="layer",
    )(
        stream,
        old_state,
        decay_amounts,
        first_gain,
        first_gate,
        first_up,
        first_down,
        mixer_gain,
        query_weight,
        key_weight,
        decay_weight,
        value_weight,
        output_gate_weight,
        head_gain,
        output_weight,
        second_gain,
        second_gate,
        second_up,
        second_down,
    )


def solution(mesh):
    in_specs = (
        P("dp", ("kv", "tp")),
        P(("dp", "kv"), "tp", None, None),
        P(("dp", "kv"), "tp"),
        P(),
        P(None, ("kv", "tp")),
        P(None, ("kv", "tp")),
        P(("kv", "tp"), None),
        P("kv"),
        P("kv", "tp"),
        P("kv", "tp"),
        P("kv", "tp"),
        P("kv", "tp"),
        P("kv", "tp"),
        P("tp"),
        P("tp", "kv"),
        P(),
        P(None, ("kv", "tp")),
        P(None, ("kv", "tp")),
        P(("kv", "tp"), None),
    )
    out_specs = (P("dp", ("kv", "tp")), P(("dp", "kv"), "tp", None, None))
    return jax.shard_map(
        functools.partial(body, mesh.shape["kv"], mesh.shape["tp"]),
        mesh=mesh,
        in_specs=in_specs,
        out_specs=out_specs,
        check_vma=False,
    )
```

```python
import functools

import jax
import jax.numpy as jnp
from jax import lax
from jax.experimental import pallas as pl
from jax.experimental.pallas import tpu as pltpu
from jax.sharding import PartitionSpec as P

EPSILON = 1e-06
GATE_SOFTNESS = 16.0
MESH = pl.DeviceIdType.MESH
F32 = jnp.float32
BF16 = jnp.bfloat16


def dot(a, b):
    return jnp.dot(a, b, preferred_element_type=F32)


def dot_t(a, b):
    return lax.dot_general(a, b, (((1,), (1,)), ((), ())), preferred_element_type=F32)


def layer_kernel(
    n_kv,
    n_tp,
    stream_h,
    state_h,
    amounts_h,
    gain1_h,
    gate1_h,
    up1_h,
    down1_h,
    mixgain_h,
    query_h,
    key_h,
    decay_h,
    value_h,
    outgate_h,
    headgain_h,
    output_h,
    gain2_h,
    gate2_h,
    up2_h,
    down2_h,
    out_ref,
    newstate_v,
    stream_v,
    state_v,
    amounts_v,
    gain1_v,
    gate1_v,
    up1_v,
    down1_v,
    mixgain_v,
    proj_v,
    headgain_v,
    output_v,
    gain2_v,
    gate2_v,
    up2_v,
    down2_v,
    wide_v,
    down_out,
    down_in,
    middle_v,
    proj_out,
    proj_in,
    mixed_v,
    attn_v,
    after_v,
    last_out,
    last_in,
    load_sem,
    a_send,
    a_recv,
    c_send,
    c_recv,
    d_send,
    d_recv,
    m_send,
    m_recv,
    e_send,
    e_recv,
    g_send,
    g_recv,
    h_send,
    h_recv,
):
    z = lax.axis_index("kv")
    c = lax.axis_index("tp")
    me = z * n_tp + c
    seqs, own_cols = stream_v.shape
    chip_cols = own_cols * n_tp
    width = chip_cols * n_kv
    rows, heads, key_dim, value_dim = state_v.shape
    key_cols = heads * key_dim
    value_cols = heads * value_dim

    loads = []

    def load(src, dst):
        copy = pltpu.make_async_copy(src, dst, load_sem.at[len(loads)])
        copy.start()
        loads.append(copy)
        return copy

    load_stream = load(stream_h, stream_v)
    load_gain1 = load(gain1_h, gain1_v)
    load_gate1 = load(gate1_h, gate1_v)
    load_up1 = load(up1_h, up1_v)
    load_down1 = load(down1_h, down1_v)

    far = []
    for j in range(n_kv - 1):
        down_t = n_kv - 1 - j
        low = jnp.where(down_t <= z, down_t - 1, down_t)
        high = jnp.where(j >= z, j + 1, j)
        far.append(jnp.where(z < n_kv // 2, low, high))
    cores = [lax.rem(c + k, n_tp) for k in range(n_tp)]
    peers = [(t, k) for t in far for k in cores] + [(z, k) for k in cores[1:]]

    barrier = pltpu.get_barrier_semaphore()
    for t, k in peers:
        pl.semaphore_signal(barrier, inc=1, device_id={"kv": t, "tp": k}, device_id_type=MESH)
    pl.semaphore_wait(barrier, len(peers))

    sent = []

    def send(src, dst, send_sem, recv_sem, t, k):
        copy = pltpu.make_async_remote_copy(
            src_ref=src,
            dst_ref=dst,
            send_sem=send_sem,
            recv_sem=recv_sem,
            device_id={"kv": t, "tp": k},
            device_id_type=MESH,
        )
        copy.start()
        sent.append(copy)

    def arrived(ref, send_sem, recv_sem, t, k):
        pltpu.make_async_remote_copy(
            src_ref=ref,
            dst_ref=ref,
            send_sem=send_sem,
            recv_sem=recv_sem,
            device_id={"kv": t, "tp": k},
            device_id_type=MESH,
        ).wait_recv()

    load_stream.wait()
    for p, (t, k) in enumerate(peers):
        send(stream_v, wide_v.at[me], a_send.at[p], a_recv.at[me], t, k)
    wide_v[me] = stream_v[...]

    load_state = load(state_h, state_v)
    load_small = [load(amounts_h, amounts_v), load(headgain_h, headgain_v)]
    load_mix = [load(mixgain_h, mixgain_v)]
    at = 0
    for ref in (query_h, key_h, decay_h, value_h, outgate_h):
        load_mix.append(load(ref, proj_v.at[:, at : at + ref.shape[1]]))
        at += ref.shape[1]
    proj_cols = at
    load_output = load(output_h, output_v)
    load_second = [load(gain2_h, gain2_v), load(gate2_h, gate2_v), load(up2_h, up2_v)]
    load_down2 = load(down2_h, down2_v)

    load_gain1.wait()
    load_gate1.wait()
    load_up1.wait()
    gate_acc = jnp.zeros((seqs, gate1_v.shape[0]), F32)
    up_acc = jnp.zeros((seqs, up1_v.shape[0]), F32)
    squares = jnp.zeros((seqs, 1), F32)
    order = [(z, k) for k in cores] + [(t, k) for t in far[::-1] for k in cores]
    for i, (t, k) in enumerate(order):
        who = t * n_tp + k
        if i:
            arrived(wide_v.at[who], a_send.at[0], a_recv.at[who], t, k)
        block = wide_v[who].astype(F32)
        cols = pl.ds(pl.multiple_of(who * own_cols, own_cols), own_cols)
        scaled = (block * gain1_v[:, cols]).astype(BF16)
        squares += jnp.sum(block * block, axis=1, keepdims=True)
        gate_acc += dot_t(scaled, gate1_v[:, cols])
        up_acc += dot_t(scaled, up1_v[:, cols])
    scale = lax.rsqrt(squares / width + EPSILON)
    hidden = (jax.nn.silu(gate_acc * scale) * (up_acc * scale)).astype(BF16)

    load_down1.wait()
    for j, t in enumerate(far):
        cols = pl.ds(pl.multiple_of(t * chip_cols, chip_cols), chip_cols)
        down_out[j] = dot(hidden, down1_v[:, cols]).astype(BF16)
        for i, k in enumerate(cores):
            send(down_out.at[j], down_in.at[me], c_send.at[j * n_tp + i], c_recv.at[me], t, k)
    cols = pl.ds(pl.multiple_of(z * chip_cols, chip_cols), chip_cols)
    own = dot(hidden, down1_v[:, cols])
    down_out[n_kv - 1] = own.astype(BF16)
    for i, k in enumerate(cores[1:]):
        send(
            down_out.at[n_kv - 1],
            down_in.at[me],
            c_send.at[(n_kv - 1) * n_tp + i],
            c_recv.at[me],
            z,
            k,
        )
    summed = own.astype(BF16).astype(F32)
    for t, k in order[1:]:
        who = t * n_tp + k
        arrived(down_in.at[who], c_send.at[0], c_recv.at[who], t, k)
        summed += down_in[who].astype(F32)
    chip_stream = jnp.concatenate([wide_v[z * n_tp + i] for i in range(n_tp)], axis=1)
    middle = (chip_stream.astype(F32) + 0.5 * summed).astype(BF16)
    middle_v[z] = middle

    for copy in load_mix:
        copy.wait()
    middle_wide = middle.astype(F32)
    scaled = (middle_wide * mixgain_v[...]).astype(BF16)
    part = dot(scaled, proj_v[...])
    square_part = jnp.broadcast_to(
        jnp.sum(middle_wide * middle_wide, axis=1, keepdims=True), (seqs, 128)
    )
    for j in range(n_kv):
        proj_out[j, :, :proj_cols] = part[j * rows : (j + 1) * rows]
        proj_out[j, :, proj_cols:] = square_part[j * rows : (j + 1) * rows]
    for j, t in enumerate(far):
        send(proj_out.at[t], proj_in.at[z], d_send.at[j], d_recv.at[z], t, c)
    for j, t in enumerate(far):
        send(middle_v.at[z], middle_v.at[z], m_send.at[j], m_recv.at[z], t, c)

    total = proj_out[z]
    for t in far[::-1]:
        arrived(proj_in.at[t], d_send.at[0], d_recv.at[t], t, c)
        total += proj_in[t]
    scale = lax.rsqrt(total[:, proj_cols : proj_cols + 1] / width + EPSILON)
    total = total[:, :proj_cols] * scale
    query = total[:, :key_cols] * key_dim ** (-0.5)
    keys = total[:, key_cols : 2 * key_cols]
    logits = total[:, 2 * key_cols : 3 * key_cols]
    values = total[:, 3 * key_cols : 3 * key_cols + value_cols]
    outgate = total[:, 3 * key_cols + value_cols :]
    for copy in load_small:
        copy.wait()
    log_sigmoid = jnp.minimum(logits, 0.0) - jnp.log(1.0 + jnp.exp(-jnp.abs(logits)))
    decay = jnp.exp(log_sigmoid / GATE_SOFTNESS - amounts_v[...])
    stacked = jnp.concatenate(
        [query, keys, decay, jnp.zeros((128 - 3 * rows, key_cols), F32)], axis=0
    )
    turned = stacked.T
    gated = headgain_v[...] * jax.nn.silu(outgate)
    load_state.wait()
    mixed_rows = []
    for b in range(rows):
        pieces = []
        for h in range(heads):
            span = slice(h * key_dim, (h + 1) * key_dim)
            lane = slice(h * value_dim, (h + 1) * value_dim)
            q_col = turned[span, b : b + 1]
            k_col = turned[span, rows + b : rows + b + 1]
            d_col = turned[span, 2 * rows + b : 2 * rows + b + 1]
            new = d_col * state_v[b, h] + k_col * values[b : b + 1, lane]
            newstate_v[b, h] = new
            readout = jnp.sum(q_col * new, axis=0, keepdims=True)
            normed = readout * lax.rsqrt(
                jnp.mean(readout * readout, axis=1, keepdims=True) + EPSILON
            )
            pieces.append(normed * gated[b : b + 1, lane])
        mixed_rows.append(jnp.concatenate(pieces, axis=1))

    mixed_v[z] = jnp.concatenate(mixed_rows, axis=0).astype(BF16).astype(F32)
    for j, t in enumerate(far):
        send(mixed_v.at[z], mixed_v.at[z], e_send.at[j], e_recv.at[z], t, c)
    load_output.wait()
    for t in far[::-1]:
        arrived(mixed_v.at[t], e_send.at[0], e_recv.at[t], t, c)
    mixed = jnp.concatenate([mixed_v[j] for j in range(n_kv)], axis=0).astype(BF16)
    attn_v[me] = dot(mixed, output_v[...]).astype(BF16)

    for p, (t, k) in enumerate(peers):
        send(attn_v.at[me], attn_v.at[me], g_send.at[p], g_recv.at[me], t, k)
    for copy in load_second:
        copy.wait()
    gate_acc = jnp.zeros((seqs, gate2_v.shape[0]), F32)
    up_acc = jnp.zeros((seqs, up2_v.shape[0]), F32)
    squares = jnp.zeros((seqs, 1), F32)
    for t in [z] + far[::-1]:
        if t is not z:
            arrived(middle_v.at[t], m_send.at[0], m_recv.at[t], t, c)
        attention = jnp.zeros((seqs, chip_cols), F32)
        for k in cores:
            who = t * n_tp + k
            if not (t is z and k is cores[0]):
                arrived(attn_v.at[who], g_send.at[0], g_recv.at[who], t, k)
            attention += attn_v[who].astype(F32)
        after = (middle_v[t].astype(F32) + attention).astype(BF16)
        block = after.astype(F32)
        if t is z:
            for i in range(n_tp):
                after_v[i] = block[:, i * own_cols : (i + 1) * own_cols]
        cols = pl.ds(pl.multiple_of(t * chip_cols, chip_cols), chip_cols)
        scaled = (block * gain2_v[:, cols]).astype(BF16)
        squares += jnp.sum(block * block, axis=1, keepdims=True)
        gate_acc += dot_t(scaled, gate2_v[:, cols])
        up_acc += dot_t(scaled, up2_v[:, cols])
    scale = lax.rsqrt(squares / width + EPSILON)
    hidden = (jax.nn.silu(gate_acc * scale) * (up_acc * scale)).astype(BF16)

    load_down2.wait()
    for j, t in enumerate(far):
        cols = pl.ds(pl.multiple_of(t * chip_cols, chip_cols), chip_cols)
        piece = dot(hidden, down2_v[:, cols]).astype(BF16)
        for k in range(n_tp):
            last_out[j, k] = piece[:, k * own_cols : (k + 1) * own_cols]
            send(last_out.at[j, k], last_in.at[me], h_send.at[j * n_tp + k], h_recv.at[me], t, k)
    cols = pl.ds(pl.multiple_of(z * chip_cols, chip_cols), chip_cols)
    piece = dot(hidden, down2_v[:, cols]).astype(BF16)
    for k in range(n_tp):
        last_out[n_kv - 1, k] = piece[:, k * own_cols : (k + 1) * own_cols]
    for i, k in enumerate(cores[1:]):
        send(
            last_out.at[n_kv - 1, k],
            last_in.at[me],
            h_send.at[(n_kv - 1) * n_tp + i],
            h_recv.at[me],
            z,
            k,
        )
    summed = last_out[n_kv - 1, c].astype(F32)
    for t, k in order[1:]:
        who = t * n_tp + k
        arrived(last_in.at[who], h_send.at[0], h_recv.at[who], t, k)
        summed += last_in[who].astype(F32)
    out_ref[...] = (after_v[c] + 0.5 * summed).astype(BF16)

    for copy in sent:
        copy.wait_send()


def half_block(stream, norm_gain, w_gate, w_up, w_down):
    wide = lax.all_gather(stream, ("kv", "tp"), axis=1, tiled=True).astype(jnp.float32)
    scaled = (wide * norm_gain).astype(jnp.bfloat16)
    gate_acc = jnp.dot(scaled, w_gate, preferred_element_type=jnp.float32)
    up_acc = jnp.dot(scaled, w_up, preferred_element_type=jnp.float32)
    square_acc = jnp.sum(wide * wide, axis=1)
    row_scale = lax.rsqrt(square_acc / norm_gain.shape[0] + EPSILON)[:, None]
    hidden = (jax.nn.silu(gate_acc * row_scale) * (up_acc * row_scale)).astype(jnp.bfloat16)
    partial_out = jnp.dot(hidden, w_down, preferred_element_type=jnp.float32)
    summed = lax.psum_scatter(partial_out, ("kv", "tp"), scatter_dimension=1, tiled=True)
    return (stream.astype(jnp.float32) + 0.5 * summed).astype(jnp.bfloat16)


def portable_body(
    stream,
    old_state,
    decay_amounts,
    first_gain,
    first_gate,
    first_up,
    first_down,
    mixer_gain,
    query_weight,
    key_weight,
    decay_weight,
    value_weight,
    output_gate_weight,
    head_gain,
    output_weight,
    second_gain,
    second_gate,
    second_up,
    second_down,
):
    middle = half_block(stream, first_gain, first_gate, first_up, first_down)
    paired_cols = lax.all_gather(middle, "tp", axis=1, tiled=True)
    wide_cols = paired_cols.astype(jnp.float32)
    scaled = (wide_cols * mixer_gain).astype(jnp.bfloat16)
    query_part = jnp.dot(scaled, query_weight, preferred_element_type=jnp.float32)
    key_part = jnp.dot(scaled, key_weight, preferred_element_type=jnp.float32)
    decay_part = jnp.dot(scaled, decay_weight, preferred_element_type=jnp.float32)
    value_part = jnp.dot(scaled, value_weight, preferred_element_type=jnp.float32)
    outgate_part = jnp.dot(scaled, output_gate_weight, preferred_element_type=jnp.float32)
    local_rows = old_state.shape[0]
    local_heads = old_state.shape[1]
    key_dim = old_state.shape[2]
    value_dim = old_state.shape[3]
    query_sum, key_sum, decay_sum, value_sum, outgate_sum, own_squares = (
        lax.psum_scatter(query_part, "kv", scatter_dimension=0, tiled=True),
        lax.psum_scatter(key_part, "kv", scatter_dimension=0, tiled=True),
        lax.psum_scatter(decay_part, "kv", scatter_dimension=0, tiled=True),
        lax.psum_scatter(value_part, "kv", scatter_dimension=0, tiled=True),
        lax.psum_scatter(outgate_part, "kv", scatter_dimension=0, tiled=True),
        lax.psum_scatter(
            jnp.sum(wide_cols * wide_cols, axis=1), "kv", scatter_dimension=0, tiled=True
        ),
    )
    row_scale = lax.rsqrt(own_squares / first_gain.shape[0] + EPSILON)[:, None]
    query = (query_sum * row_scale * key_dim ** (-0.5)).reshape(local_rows, local_heads, key_dim)
    keys = (key_sum * row_scale).reshape(local_rows, local_heads, key_dim)
    gate_logits = (decay_sum * row_scale).reshape(local_rows, local_heads, key_dim)
    values = (value_sum * row_scale).reshape(local_rows, local_heads, value_dim)
    decay_logarithm = jax.nn.log_sigmoid(gate_logits) / GATE_SOFTNESS - decay_amounts.reshape(
        local_rows, local_heads, key_dim
    )
    new_state = (
        jnp.exp(decay_logarithm)[..., None] * old_state + keys[..., None] * values[:, :, None, :]
    )
    readout = jnp.einsum("bhk,bhkv->bhv", query, new_state, precision=lax.Precision.HIGHEST)
    normed = readout * lax.rsqrt(jnp.mean(readout * readout, axis=-1, keepdims=True) + EPSILON)
    mixed_heads = (
        normed.reshape(local_rows, local_heads * value_dim)
        * head_gain
        * jax.nn.silu(outgate_sum * row_scale)
    ).astype(jnp.bfloat16)
    projected = jnp.dot(
        lax.all_gather(mixed_heads, "kv", axis=0, tiled=True),
        output_weight,
        preferred_element_type=jnp.float32,
    ).astype(jnp.bfloat16)
    attention_out = lax.psum_scatter(
        lax.optimization_barrier(projected).astype(jnp.float32).astype(jnp.bfloat16),
        "tp",
        scatter_dimension=1,
        tiled=True,
    ).astype(jnp.float32)
    after = (middle.astype(jnp.float32) + attention_out).astype(jnp.bfloat16)
    mixed_stream = half_block(after, second_gain, second_gate, second_up, second_down)
    return (mixed_stream, new_state)


def body(n_kv, n_tp, *args):
    (
        stream,
        old_state,
        decay_amounts,
        first_gain,
        first_gate,
        first_up,
        first_down,
        mixer_gain,
        query_weight,
        key_weight,
        decay_weight,
        value_weight,
        output_gate_weight,
        head_gain,
        output_weight,
        second_gain,
        second_gate,
        second_up,
        second_down,
    ) = args
    seqs, own_cols = stream.shape
    chip_cols = own_cols * n_tp
    rows, heads, key_dim, value_dim = old_state.shape
    if own_cols % 128 or value_dim % 128 or 3 * rows > 128 or n_kv * n_tp > 16:
        return portable_body(*args)
    proj_cols = 3 * heads * key_dim + 2 * heads * value_dim
    n = n_kv * n_tp
    first_gain, mixer_gain, head_gain, second_gain = (
        g.reshape(1, -1) for g in (first_gain, mixer_gain, head_gain, second_gain)
    )

    first_gate, first_up, second_gate, second_up = (
        w.T for w in (first_gate, first_up, second_gate, second_up)
    )

    def like(array):
        return pltpu.VMEM(array.shape, array.dtype)

    dma = pltpu.SemaphoreType.DMA
    scratch = [
        like(stream),
        like(old_state),
        like(decay_amounts),
        like(first_gain),
        like(first_gate),
        like(first_up),
        like(first_down),
        like(mixer_gain),
        pltpu.VMEM((chip_cols, proj_cols), BF16),
        like(head_gain),
        like(output_weight),
        like(second_gain),
        like(second_gate),
        like(second_up),
        like(second_down),
        pltpu.VMEM((n, seqs, own_cols), BF16),
        pltpu.VMEM((n_kv, seqs, chip_cols), BF16),
        pltpu.VMEM((n, seqs, chip_cols), BF16),
        pltpu.VMEM((n_kv, seqs, chip_cols), BF16),
        pltpu.VMEM((n_kv, rows, proj_cols + 128), F32),
        pltpu.VMEM((n_kv, rows, proj_cols + 128), F32),
        pltpu.VMEM((n_kv, rows, heads * value_dim), F32),
        pltpu.VMEM((n, seqs, chip_cols), BF16),
        pltpu.VMEM((n_tp, seqs, own_cols), F32),
        pltpu.VMEM((n_kv, n_tp, seqs, own_cols), BF16),
        pltpu.VMEM((n, seqs, own_cols), BF16),
        dma((19,)),
        dma((n,)),
        dma((n,)),
        dma((n,)),
        dma((n,)),
        dma((n_kv,)),
        dma((n_kv,)),
        dma((n_kv,)),
        dma((n_kv,)),
        dma((n_kv,)),
        dma((n_kv,)),
        dma((n,)),
        dma((n,)),
        dma((n,)),
        dma((n,)),
    ]
    return pl.pallas_call(
        functools.partial(layer_kernel, n_kv, n_tp),
        out_shape=(
            pltpu.VMEM(stream.shape, stream.dtype),
            pltpu.VMEM(old_state.shape, old_state.dtype),
        ),
        in_specs=[pl.BlockSpec(memory_space=pl.ANY)] * 19,
        out_specs=(
            pl.BlockSpec(memory_space=pltpu.VMEM),
            pl.BlockSpec(memory_space=pltpu.VMEM),
        ),
        scratch_shapes=scratch,
        compiler_params=pltpu.CompilerParams(
            collective_id=0, has_side_effects=True, vmem_limit_bytes=60 * 1024 * 1024
        ),
        name="layer",
    )(
        stream,
        old_state,
        decay_amounts,
        first_gain,
        first_gate,
        first_up,
        first_down,
        mixer_gain,
        query_weight,
        key_weight,
        decay_weight,
        value_weight,
        output_gate_weight,
        head_gain,
        output_weight,
        second_gain,
        second_gate,
        second_up,
        second_down,
    )


def solution(mesh):
    in_specs = (
        P("dp", ("kv", "tp")),
        P(("dp", "kv"), "tp", None, None),
        P(("dp", "kv"), "tp"),
        P(),
        P(None, ("kv", "tp")),
        P(None, ("kv", "tp")),
        P(("kv", "tp"), None),
        P("kv"),
        P("kv", "tp"),
        P("kv", "tp"),
        P("kv", "tp"),
        P("kv", "tp"),
        P("kv", "tp"),
        P("tp"),
        P("tp", "kv"),
        P(),
        P(None, ("kv", "tp")),
        P(None, ("kv", "tp")),
        P(("kv", "tp"), None),
    )
    out_specs = (P("dp", ("kv", "tp")), P(("dp", "kv"), "tp", None, None))
    return jax.shard_map(
        functools.partial(body, mesh.shape["kv"], mesh.shape["tp"]),
        mesh=mesh,
        in_specs=in_specs,
        out_specs=out_specs,
        check_vma=False,
    )
```

```python
import functools

import jax
import jax.numpy as jnp
from jax import lax
from jax.experimental import pallas as pl
from jax.experimental.pallas import tpu as pltpu
from jax.sharding import PartitionSpec as P

EPSILON = 1e-06
GATE_SOFTNESS = 16.0
MESH = pl.DeviceIdType.MESH
F32 = jnp.float32
BF16 = jnp.bfloat16


def dot(a, b):
    return jnp.dot(a, b, preferred_element_type=F32)


def dot_t(a, b):
    return lax.dot_general(a, b, (((1,), (1,)), ((), ())), preferred_element_type=F32)


def layer_kernel(
    n_kv,
    n_tp,
    stream_h,
    state_h,
    amounts_h,
    gain1_h,
    gate1_h,
    up1_h,
    down1_h,
    mixgain_h,
    query_h,
    key_h,
    decay_h,
    value_h,
    outgate_h,
    headgain_h,
    output_h,
    gain2_h,
    gate2_h,
    up2_h,
    down2_h,
    out_ref,
    newstate_v,
    stream_v,
    state_v,
    amounts_v,
    gain1_v,
    gate1_v,
    up1_v,
    down1_v,
    mixgain_v,
    proj_v,
    headgain_v,
    output_v,
    gain2_v,
    gate2_v,
    up2_v,
    down2_v,
    wide_v,
    down_out,
    down_in,
    middle_v,
    proj_out,
    proj_in,
    mixed_v,
    attn_v,
    after_v,
    last_out,
    last_in,
    load_sem,
    a_send,
    a_recv,
    c_send,
    c_recv,
    d_send,
    d_recv,
    m_send,
    m_recv,
    e_send,
    e_recv,
    g_send,
    g_recv,
    h_send,
    h_recv,
):
    z = lax.axis_index("kv")
    c = lax.axis_index("tp")
    me = z * n_tp + c
    seqs, own_cols = stream_v.shape
    chip_cols = own_cols * n_tp
    width = chip_cols * n_kv
    rows, heads, key_dim, value_dim = state_v.shape
    key_cols = heads * key_dim
    value_cols = heads * value_dim

    loads = []

    def load(src, dst):
        copy = pltpu.make_async_copy(src, dst, load_sem.at[len(loads)])
        copy.start()
        loads.append(copy)
        return copy

    load_stream = load(stream_h, stream_v)
    load_gain1 = load(gain1_h, gain1_v)
    load_gate1 = load(gate1_h, gate1_v)
    load_up1 = load(up1_h, up1_v)
    load_down1 = load(down1_h, down1_v)

    far = []
    for j in range(n_kv - 1):
        down_t = n_kv - 1 - j
        low = jnp.where(down_t <= z, down_t - 1, down_t)
        high = jnp.where(j >= z, j + 1, j)
        far.append(jnp.where(z < n_kv // 2, low, high))
    cores = [lax.rem(c + k, n_tp) for k in range(n_tp)]
    peers = [(t, k) for t in far for k in cores] + [(z, k) for k in cores[1:]]

    barrier = pltpu.get_barrier_semaphore()
    for t, k in peers:
        pl.semaphore_signal(barrier, inc=1, device_id={"kv": t, "tp": k}, device_id_type=MESH)
    pl.semaphore_wait(barrier, len(peers))

    sent = []

    def send(src, dst, send_sem, recv_sem, t, k):
        copy = pltpu.make_async_remote_copy(
            src_ref=src,
            dst_ref=dst,
            send_sem=send_sem,
            recv_sem=recv_sem,
            device_id={"kv": t, "tp": k},
            device_id_type=MESH,
        )
        copy.start()
        sent.append(copy)

    def arrived(ref, send_sem, recv_sem, t, k):
        pltpu.make_async_remote_copy(
            src_ref=ref,
            dst_ref=ref,
            send_sem=send_sem,
            recv_sem=recv_sem,
            device_id={"kv": t, "tp": k},
            device_id_type=MESH,
        ).wait_recv()

    load_stream.wait()
    for p, (t, k) in enumerate(peers):
        send(stream_v, wide_v.at[me], a_send.at[p], a_recv.at[me], t, k)
    wide_v[me] = stream_v[...]

    load_state = load(state_h, state_v)
    load_small = [load(amounts_h, amounts_v), load(headgain_h, headgain_v)]
    load_mix = [load(mixgain_h, mixgain_v)]
    at = 0
    for ref in (query_h, key_h, decay_h, value_h, outgate_h):
        load_mix.append(load(ref, proj_v.at[:, at : at + ref.shape[1]]))
        at += ref.shape[1]
    load_output = load(output_h, output_v)
    load_second = [load(gain2_h, gain2_v), load(gate2_h, gate2_v), load(up2_h, up2_v)]
    load_down2 = load(down2_h, down2_v)

    load_gain1.wait()
    load_gate1.wait()
    load_up1.wait()
    gate_acc = jnp.zeros((seqs, gate1_v.shape[0]), F32)
    up_acc = jnp.zeros((seqs, up1_v.shape[0]), F32)
    squares = jnp.zeros((seqs, 1), F32)
    order = [(z, k) for k in cores] + [(t, k) for t in far[::-1] for k in cores]
    for i, (t, k) in enumerate(order):
        who = t * n_tp + k
        if i:
            arrived(wide_v.at[who], a_send.at[0], a_recv.at[who], t, k)
        block = wide_v[who].astype(F32)
        cols = pl.ds(pl.multiple_of(who * own_cols, own_cols), own_cols)
        scaled = (block * gain1_v[:, cols]).astype(BF16)
        squares += jnp.sum(block * block, axis=1, keepdims=True)
        gate_acc += dot_t(scaled, gate1_v[:, cols])
        up_acc += dot_t(scaled, up1_v[:, cols])
    scale = lax.rsqrt(squares / width + EPSILON)
    hidden = (jax.nn.silu(gate_acc * scale) * (up_acc * scale)).astype(BF16)

    load_down1.wait()
    for j, t in enumerate(far):
        cols = pl.ds(pl.multiple_of(t * chip_cols, chip_cols), chip_cols)
        down_out[j] = dot(hidden, down1_v[:, cols]).astype(BF16)
        for i, k in enumerate(cores):
            send(down_out.at[j], down_in.at[me], c_send.at[j * n_tp + i], c_recv.at[me], t, k)
    cols = pl.ds(pl.multiple_of(z * chip_cols, chip_cols), chip_cols)
    own = dot(hidden, down1_v[:, cols])
    down_out[n_kv - 1] = own.astype(BF16)
    for i, k in enumerate(cores[1:]):
        send(
            down_out.at[n_kv - 1],
            down_in.at[me],
            c_send.at[(n_kv - 1) * n_tp + i],
            c_recv.at[me],
            z,
            k,
        )
    summed = own.astype(BF16).astype(F32)
    for t, k in order[1:]:
        who = t * n_tp + k
        arrived(down_in.at[who], c_send.at[0], c_recv.at[who], t, k)
        summed += down_in[who].astype(F32)
    chip_stream = jnp.concatenate([wide_v[z * n_tp + i] for i in range(n_tp)], axis=1)
    middle = (chip_stream.astype(F32) + 0.5 * summed).astype(BF16)
    middle_v[z] = middle

    for copy in load_mix:
        copy.wait()
    middle_wide = middle.astype(F32)
    scaled = (middle_wide * mixgain_v[...]).astype(BF16)
    part = dot(scaled, proj_v[...])
    square_part = jnp.broadcast_to(
        jnp.sum(middle_wide * middle_wide, axis=1, keepdims=True), (seqs, key_cols)
    )
    queries_keys = part[:, : 2 * key_cols]
    logits_squares = jnp.concatenate([part[:, 2 * key_cols : 3 * key_cols], square_part], axis=1)
    values_part = part[:, 3 * key_cols : 3 * key_cols + value_cols]
    gates_part = part[:, 3 * key_cols + value_cols :]
    for j in range(n_kv):
        mine = slice(j * rows, (j + 1) * rows)
        proj_out[j] = jnp.concatenate(
            [queries_keys[mine], logits_squares[mine], values_part[mine], gates_part[mine]], axis=0
        )
    for j, t in enumerate(far):
        send(proj_out.at[t], proj_in.at[z], d_send.at[j], d_recv.at[z], t, c)
    for j, t in enumerate(far):
        send(middle_v.at[z], middle_v.at[z], m_send.at[j], m_recv.at[z], t, c)

    for copy in load_small:
        copy.wait()
    load_state.wait()
    load_output.wait()
    total = proj_out[z]
    for t in far[::-1]:
        arrived(proj_in.at[t], d_send.at[0], d_recv.at[t], t, c)
        total += proj_in[t]
    scale = lax.rsqrt(total[rows : 2 * rows, key_cols : key_cols + 1] / width + EPSILON)
    query = total[:rows, :key_cols] * (scale * key_dim ** (-0.5))
    keys = total[:rows, key_cols:] * scale
    logits = total[rows : 2 * rows, :key_cols] * scale
    values = total[2 * rows : 3 * rows] * scale
    outgate = total[3 * rows :] * scale
    log_sigmoid = jnp.minimum(logits, 0.0) - jnp.log(1.0 + jnp.exp(-jnp.abs(logits)))
    decay = jnp.exp(log_sigmoid / GATE_SOFTNESS - amounts_v[...])
    stacked = jnp.concatenate(
        [query, keys, decay, jnp.zeros((-3 * rows % 8, key_cols), F32)], axis=0
    )
    turned = stacked.T
    gated = headgain_v[...] * jax.nn.silu(outgate)
    readouts, gates = [], []
    for h in range(heads):
        span = slice(h * key_dim, (h + 1) * key_dim)
        lane = slice(h * value_dim, (h + 1) * value_dim)
        gates.append(gated[:, lane])
        for b in range(rows):
            q_col = turned[span, b : b + 1]
            k_col = turned[span, rows + b : rows + b + 1]
            d_col = turned[span, 2 * rows + b : 2 * rows + b + 1]
            new = d_col * state_v[b, h] + k_col * values[b : b + 1, lane]
            newstate_v[b, h] = new
            readouts.append(jnp.sum(q_col * new, axis=0, keepdims=True))
    readout = jnp.concatenate(readouts, axis=0)
    normed = readout * lax.rsqrt(jnp.mean(readout * readout, axis=1, keepdims=True) + EPSILON)

    mixed_v[z] = (normed * jnp.concatenate(gates, axis=0)).astype(BF16).astype(F32)
    for j, t in enumerate(far):
        send(mixed_v.at[z], mixed_v.at[z], e_send.at[j], e_recv.at[z], t, c)
    for t in far[::-1]:
        arrived(mixed_v.at[t], e_send.at[0], e_recv.at[t], t, c)
    blocks = [mixed_v[j] for j in range(n_kv)]
    mixed = jnp.concatenate(
        [
            jnp.concatenate([block[h * rows : (h + 1) * rows] for block in blocks], axis=0)
            for h in range(heads)
        ],
        axis=1,
    ).astype(BF16)
    attn_v[me] = dot(mixed, output_v[...]).astype(BF16)

    for p, (t, k) in enumerate(peers):
        send(attn_v.at[me], attn_v.at[me], g_send.at[p], g_recv.at[me], t, k)
    for copy in load_second:
        copy.wait()
    gate_acc = jnp.zeros((seqs, gate2_v.shape[0]), F32)
    up_acc = jnp.zeros((seqs, up2_v.shape[0]), F32)
    squares = jnp.zeros((seqs, 1), F32)
    for t in [z] + far[::-1]:
        if t is not z:
            arrived(middle_v.at[t], m_send.at[0], m_recv.at[t], t, c)
        attention = jnp.zeros((seqs, chip_cols), F32)
        for k in cores:
            who = t * n_tp + k
            if not (t is z and k is cores[0]):
                arrived(attn_v.at[who], g_send.at[0], g_recv.at[who], t, k)
            attention += attn_v[who].astype(F32)
        after = (middle_v[t].astype(F32) + attention).astype(BF16)
        block = after.astype(F32)
        if t is z:
            for i in range(n_tp):
                after_v[i] = block[:, i * own_cols : (i + 1) * own_cols]
        cols = pl.ds(pl.multiple_of(t * chip_cols, chip_cols), chip_cols)
        scaled = (block * gain2_v[:, cols]).astype(BF16)
        squares += jnp.sum(block * block, axis=1, keepdims=True)
        gate_acc += dot_t(scaled, gate2_v[:, cols])
        up_acc += dot_t(scaled, up2_v[:, cols])
    scale = lax.rsqrt(squares / width + EPSILON)
    hidden = (jax.nn.silu(gate_acc * scale) * (up_acc * scale)).astype(BF16)

    load_down2.wait()
    for j, t in enumerate(far):
        cols = pl.ds(pl.multiple_of(t * chip_cols, chip_cols), chip_cols)
        piece = dot(hidden, down2_v[:, cols]).astype(BF16)
        for k in range(n_tp):
            last_out[j, k] = piece[:, k * own_cols : (k + 1) * own_cols]
            send(last_out.at[j, k], last_in.at[me], h_send.at[j * n_tp + k], h_recv.at[me], t, k)
    cols = pl.ds(pl.multiple_of(z * chip_cols, chip_cols), chip_cols)
    piece = dot(hidden, down2_v[:, cols]).astype(BF16)
    for k in range(n_tp):
        last_out[n_kv - 1, k] = piece[:, k * own_cols : (k + 1) * own_cols]
    for i, k in enumerate(cores[1:]):
        send(
            last_out.at[n_kv - 1, k],
            last_in.at[me],
            h_send.at[(n_kv - 1) * n_tp + i],
            h_recv.at[me],
            z,
            k,
        )
    summed = last_out[n_kv - 1, c].astype(F32)
    for t, k in order[1:]:
        who = t * n_tp + k
        arrived(last_in.at[who], h_send.at[0], h_recv.at[who], t, k)
        summed += last_in[who].astype(F32)
    out_ref[...] = (after_v[c] + 0.5 * summed).astype(BF16)

    for copy in sent:
        copy.wait_send()


def store_kernel(stream_v, state_v, stream_h, state_h, sem):
    copies = [
        pltpu.make_async_copy(state_v, state_h, sem.at[0]),
        pltpu.make_async_copy(stream_v, stream_h, sem.at[1]),
    ]
    for copy in copies:
        copy.start()
    for copy in copies:
        copy.wait()


def half_block(stream, norm_gain, w_gate, w_up, w_down):
    wide = lax.all_gather(stream, ("kv", "tp"), axis=1, tiled=True).astype(jnp.float32)
    scaled = (wide * norm_gain).astype(jnp.bfloat16)
    gate_acc = jnp.dot(scaled, w_gate, preferred_element_type=jnp.float32)
    up_acc = jnp.dot(scaled, w_up, preferred_element_type=jnp.float32)
    square_acc = jnp.sum(wide * wide, axis=1)
    row_scale = lax.rsqrt(square_acc / norm_gain.shape[0] + EPSILON)[:, None]
    hidden = (jax.nn.silu(gate_acc * row_scale) * (up_acc * row_scale)).astype(jnp.bfloat16)
    partial_out = jnp.dot(hidden, w_down, preferred_element_type=jnp.float32)
    summed = lax.psum_scatter(partial_out, ("kv", "tp"), scatter_dimension=1, tiled=True)
    return (stream.astype(jnp.float32) + 0.5 * summed).astype(jnp.bfloat16)


def portable_body(
    stream,
    old_state,
    decay_amounts,
    first_gain,
    first_gate,
    first_up,
    first_down,
    mixer_gain,
    query_weight,
    key_weight,
    decay_weight,
    value_weight,
    output_gate_weight,
    head_gain,
    output_weight,
    second_gain,
    second_gate,
    second_up,
    second_down,
):
    middle = half_block(stream, first_gain, first_gate, first_up, first_down)
    paired_cols = lax.all_gather(middle, "tp", axis=1, tiled=True)
    wide_cols = paired_cols.astype(jnp.float32)
    scaled = (wide_cols * mixer_gain).astype(jnp.bfloat16)
    query_part = jnp.dot(scaled, query_weight, preferred_element_type=jnp.float32)
    key_part = jnp.dot(scaled, key_weight, preferred_element_type=jnp.float32)
    decay_part = jnp.dot(scaled, decay_weight, preferred_element_type=jnp.float32)
    value_part = jnp.dot(scaled, value_weight, preferred_element_type=jnp.float32)
    outgate_part = jnp.dot(scaled, output_gate_weight, preferred_element_type=jnp.float32)
    local_rows = old_state.shape[0]
    local_heads = old_state.shape[1]
    key_dim = old_state.shape[2]
    value_dim = old_state.shape[3]
    query_sum, key_sum, decay_sum, value_sum, outgate_sum, own_squares = (
        lax.psum_scatter(query_part, "kv", scatter_dimension=0, tiled=True),
        lax.psum_scatter(key_part, "kv", scatter_dimension=0, tiled=True),
        lax.psum_scatter(decay_part, "kv", scatter_dimension=0, tiled=True),
        lax.psum_scatter(value_part, "kv", scatter_dimension=0, tiled=True),
        lax.psum_scatter(outgate_part, "kv", scatter_dimension=0, tiled=True),
        lax.psum_scatter(
            jnp.sum(wide_cols * wide_cols, axis=1), "kv", scatter_dimension=0, tiled=True
        ),
    )
    row_scale = lax.rsqrt(own_squares / first_gain.shape[0] + EPSILON)[:, None]
    query = (query_sum * row_scale * key_dim ** (-0.5)).reshape(local_rows, local_heads, key_dim)
    keys = (key_sum * row_scale).reshape(local_rows, local_heads, key_dim)
    gate_logits = (decay_sum * row_scale).reshape(local_rows, local_heads, key_dim)
    values = (value_sum * row_scale).reshape(local_rows, local_heads, value_dim)
    decay_logarithm = jax.nn.log_sigmoid(gate_logits) / GATE_SOFTNESS - decay_amounts.reshape(
        local_rows, local_heads, key_dim
    )
    new_state = (
        jnp.exp(decay_logarithm)[..., None] * old_state + keys[..., None] * values[:, :, None, :]
    )
    readout = jnp.einsum("bhk,bhkv->bhv", query, new_state, precision=lax.Precision.HIGHEST)
    normed = readout * lax.rsqrt(jnp.mean(readout * readout, axis=-1, keepdims=True) + EPSILON)
    mixed_heads = (
        normed.reshape(local_rows, local_heads * value_dim)
        * head_gain
        * jax.nn.silu(outgate_sum * row_scale)
    ).astype(jnp.bfloat16)
    projected = jnp.dot(
        lax.all_gather(mixed_heads, "kv", axis=0, tiled=True),
        output_weight,
        preferred_element_type=jnp.float32,
    ).astype(jnp.bfloat16)
    attention_out = lax.psum_scatter(
        lax.optimization_barrier(projected).astype(jnp.float32).astype(jnp.bfloat16),
        "tp",
        scatter_dimension=1,
        tiled=True,
    ).astype(jnp.float32)
    after = (middle.astype(jnp.float32) + attention_out).astype(jnp.bfloat16)
    mixed_stream = half_block(after, second_gain, second_gate, second_up, second_down)
    return (mixed_stream, new_state)


def body(n_kv, n_tp, *args):
    (
        stream,
        old_state,
        decay_amounts,
        first_gain,
        first_gate,
        first_up,
        first_down,
        mixer_gain,
        query_weight,
        key_weight,
        decay_weight,
        value_weight,
        output_gate_weight,
        head_gain,
        output_weight,
        second_gain,
        second_gate,
        second_up,
        second_down,
    ) = args
    seqs, own_cols = stream.shape
    chip_cols = own_cols * n_tp
    rows, heads, key_dim, value_dim = old_state.shape
    if own_cols % 128 or value_dim != 2 * key_dim or value_dim % 128 or n_kv * n_tp > 16:
        return portable_body(*args)
    proj_cols = 3 * heads * key_dim + 2 * heads * value_dim
    n = n_kv * n_tp
    first_gain, mixer_gain, head_gain, second_gain = (
        g.reshape(1, -1) for g in (first_gain, mixer_gain, head_gain, second_gain)
    )

    first_gate, first_up, second_gate, second_up = (
        w.T for w in (first_gate, first_up, second_gate, second_up)
    )

    def like(array):
        return pltpu.VMEM(array.shape, array.dtype)

    dma = pltpu.SemaphoreType.DMA
    scratch = [
        like(stream),
        like(old_state),
        like(decay_amounts),
        like(first_gain),
        like(first_gate),
        like(first_up),
        like(first_down),
        like(mixer_gain),
        pltpu.VMEM((chip_cols, proj_cols), BF16),
        like(head_gain),
        like(output_weight),
        like(second_gain),
        like(second_gate),
        like(second_up),
        like(second_down),
        pltpu.VMEM((n, seqs, own_cols), BF16),
        pltpu.VMEM((n_kv, seqs, chip_cols), BF16),
        pltpu.VMEM((n, seqs, chip_cols), BF16),
        pltpu.VMEM((n_kv, seqs, chip_cols), BF16),
        pltpu.VMEM((n_kv, 4 * rows, heads * value_dim), F32),
        pltpu.VMEM((n_kv, 4 * rows, heads * value_dim), F32),
        pltpu.VMEM((n_kv, heads * rows, value_dim), F32),
        pltpu.VMEM((n, seqs, chip_cols), BF16),
        pltpu.VMEM((n_tp, seqs, own_cols), F32),
        pltpu.VMEM((n_kv, n_tp, seqs, own_cols), BF16),
        pltpu.VMEM((n, seqs, own_cols), BF16),
        dma((19,)),
        dma((n,)),
        dma((n,)),
        dma((n,)),
        dma((n,)),
        dma((n_kv,)),
        dma((n_kv,)),
        dma((n_kv,)),
        dma((n_kv,)),
        dma((n_kv,)),
        dma((n_kv,)),
        dma((n,)),
        dma((n,)),
        dma((n,)),
        dma((n,)),
    ]
    mixed_stream, new_state = pl.pallas_call(
        functools.partial(layer_kernel, n_kv, n_tp),
        out_shape=(
            pltpu.VMEM(stream.shape, stream.dtype),
            pltpu.VMEM(old_state.shape, old_state.dtype),
        ),
        in_specs=[pl.BlockSpec(memory_space=pl.ANY)] * 19,
        out_specs=(
            pl.BlockSpec(memory_space=pltpu.VMEM),
            pl.BlockSpec(memory_space=pltpu.VMEM),
        ),
        scratch_shapes=scratch,
        compiler_params=pltpu.CompilerParams(
            collective_id=0, has_side_effects=True, vmem_limit_bytes=60 * 1024 * 1024
        ),
        name="layer",
    )(
        stream,
        old_state,
        decay_amounts,
        first_gain,
        first_gate,
        first_up,
        first_down,
        mixer_gain,
        query_weight,
        key_weight,
        decay_weight,
        value_weight,
        output_gate_weight,
        head_gain,
        output_weight,
        second_gain,
        second_gate,
        second_up,
        second_down,
    )
    return pl.pallas_call(
        store_kernel,
        out_shape=(
            jax.ShapeDtypeStruct(stream.shape, stream.dtype),
            jax.ShapeDtypeStruct(old_state.shape, old_state.dtype),
        ),
        in_specs=[pl.BlockSpec(memory_space=pltpu.VMEM)] * 2,
        out_specs=(pl.BlockSpec(memory_space=pl.ANY),) * 2,
        scratch_shapes=[dma((2,))],
        name="store",
    )(
        pltpu.with_memory_space_constraint(mixed_stream, pltpu.VMEM),
        pltpu.with_memory_space_constraint(new_state, pltpu.VMEM),
    )


def solution(mesh):
    in_specs = (
        P("dp", ("kv", "tp")),
        P(("dp", "kv"), "tp", None, None),
        P(("dp", "kv"), "tp"),
        P(),
        P(None, ("kv", "tp")),
        P(None, ("kv", "tp")),
        P(("kv", "tp"), None),
        P("kv"),
        P("kv", "tp"),
        P("kv", "tp"),
        P("kv", "tp"),
        P("kv", "tp"),
        P("kv", "tp"),
        P("tp"),
        P("tp", "kv"),
        P(),
        P(None, ("kv", "tp")),
        P(None, ("kv", "tp")),
        P(("kv", "tp"), None),
    )
    out_specs = (P("dp", ("kv", "tp")), P(("dp", "kv"), "tp", None, None))
    return jax.shard_map(
        functools.partial(body, mesh.shape["kv"], mesh.shape["tp"]),
        mesh=mesh,
        in_specs=in_specs,
        out_specs=out_specs,
        check_vma=False,
    )
```

```python
import functools

import jax
import jax.numpy as jnp
from jax import lax
from jax.experimental import pallas as pl
from jax.experimental.pallas import tpu as pltpu
from jax.sharding import PartitionSpec as P

EPSILON = 1e-06
GATE_SOFTNESS = 16.0
MESH = pl.DeviceIdType.MESH
F32 = jnp.float32
BF16 = jnp.bfloat16


def dot(a, b):
    return jnp.dot(a, b, preferred_element_type=F32)


def dot_t(a, b):
    return lax.dot_general(a, b, (((1,), (1,)), ((), ())), preferred_element_type=F32)


def layer_kernel(
    n_kv,
    n_tp,
    stream_h,
    state_h,
    amounts_h,
    gain1_h,
    gate1_h,
    up1_h,
    down1_h,
    mixgain_h,
    query_h,
    key_h,
    decay_h,
    value_h,
    outgate_h,
    headgain_h,
    output_h,
    gain2_h,
    gate2_h,
    up2_h,
    down2_h,
    out_ref,
    newstate_v,
    stream_v,
    state_v,
    amounts_v,
    gain1_v,
    gate1_v,
    up1_v,
    down1_v,
    mixgain_v,
    proj_v,
    headgain_v,
    output_v,
    gain2_v,
    gate2_v,
    up2_v,
    down2_v,
    wide_v,
    down_out,
    down_in,
    middle_v,
    proj_out,
    proj_in,
    mixed_v,
    attn_v,
    after_v,
    last_out,
    last_in,
    load_sem,
    a_send,
    a_recv,
    c_send,
    c_recv,
    d_send,
    d_recv,
    m_send,
    m_recv,
    e_send,
    e_recv,
    g_send,
    g_recv,
    h_send,
    h_recv,
):
    z = lax.axis_index("kv")
    c = lax.axis_index("tp")
    me = z * n_tp + c
    seqs, own_cols = stream_v.shape
    chip_cols = own_cols * n_tp
    width = chip_cols * n_kv
    rows, heads, key_dim, value_dim = state_v.shape
    key_cols = heads * key_dim
    value_cols = heads * value_dim

    loads = []

    def load(src, dst):
        copy = pltpu.make_async_copy(src, dst, load_sem.at[len(loads)])
        copy.start()
        loads.append(copy)
        return copy

    load_stream = load(stream_h, stream_v)

    far = []
    for j in range(n_kv - 1):
        down_t = n_kv - 1 - j
        low = jnp.where(down_t <= z, down_t - 1, down_t)
        high = jnp.where(j >= z, j + 1, j)
        far.append(jnp.where(z < n_kv // 2, low, high))
    cores = [lax.rem(c + k, n_tp) for k in range(n_tp)]
    peers = [(t, k) for t in far for k in cores] + [(z, k) for k in cores[1:]]

    barrier = pltpu.get_barrier_semaphore()
    for t, k in peers:
        pl.semaphore_signal(barrier, inc=1, device_id={"kv": t, "tp": k}, device_id_type=MESH)
    load_gain1 = load(gain1_h, gain1_v)
    load_gate1 = load(gate1_h, gate1_v)
    load_up1 = load(up1_h, up1_v)
    load_down1 = load(down1_h, down1_v)
    pl.semaphore_wait(barrier, len(peers))

    sent = []

    def send(src, dst, send_sem, recv_sem, t, k):
        copy = pltpu.make_async_remote_copy(
            src_ref=src,
            dst_ref=dst,
            send_sem=send_sem,
            recv_sem=recv_sem,
            device_id={"kv": t, "tp": k},
            device_id_type=MESH,
        )
        copy.start()
        sent.append(copy)

    def arrived(ref, send_sem, recv_sem, t, k):
        pltpu.make_async_remote_copy(
            src_ref=ref,
            dst_ref=ref,
            send_sem=send_sem,
            recv_sem=recv_sem,
            device_id={"kv": t, "tp": k},
            device_id_type=MESH,
        ).wait_recv()

    load_stream.wait()
    for p, (t, k) in enumerate(peers):
        send(stream_v, wide_v.at[me], a_send.at[p], a_recv.at[me], t, k)
    wide_v[me] = stream_v[...]

    load_state = load(state_h, state_v)
    load_small = [load(amounts_h, amounts_v), load(headgain_h, headgain_v)]
    load_mix = [load(mixgain_h, mixgain_v)]
    at = 0
    for ref in (query_h, key_h, decay_h, value_h, outgate_h):
        load_mix.append(load(ref, proj_v.at[:, at : at + ref.shape[1]]))
        at += ref.shape[1]
    load_output = load(output_h, output_v)
    load_second = [load(gain2_h, gain2_v), load(gate2_h, gate2_v), load(up2_h, up2_v)]
    load_down2 = load(down2_h, down2_v)

    load_gain1.wait()
    load_gate1.wait()
    load_up1.wait()
    gate_acc = jnp.zeros((seqs, gate1_v.shape[0]), F32)
    up_acc = jnp.zeros((seqs, up1_v.shape[0]), F32)
    squares = jnp.zeros((seqs, 1), F32)
    order = [(z, k) for k in cores] + [(t, k) for t in far[::-1] for k in cores]
    for i, (t, k) in enumerate(order):
        who = t * n_tp + k
        if i:
            arrived(wide_v.at[who], a_send.at[0], a_recv.at[who], t, k)
        block = wide_v[who].astype(F32)
        cols = pl.ds(pl.multiple_of(who * own_cols, own_cols), own_cols)
        scaled = (block * gain1_v[:, cols]).astype(BF16)
        squares += jnp.sum(block * block, axis=1, keepdims=True)
        gate_acc += dot_t(scaled, gate1_v[:, cols])
        up_acc += dot_t(scaled, up1_v[:, cols])
    scale = lax.rsqrt(squares / width + EPSILON)
    hidden = (jax.nn.silu(gate_acc * scale) * (up_acc * scale)).astype(BF16)

    load_down1.wait()
    for j, t in enumerate(far):
        cols = pl.ds(pl.multiple_of(t * chip_cols, chip_cols), chip_cols)
        down_out[j] = dot(hidden, down1_v[:, cols]).astype(BF16)
        for i, k in enumerate(cores):
            send(down_out.at[j], down_in.at[me], c_send.at[j * n_tp + i], c_recv.at[me], t, k)
    cols = pl.ds(pl.multiple_of(z * chip_cols, chip_cols), chip_cols)
    own = dot(hidden, down1_v[:, cols])
    down_out[n_kv - 1] = own.astype(BF16)
    for i, k in enumerate(cores[1:]):
        send(
            down_out.at[n_kv - 1],
            down_in.at[me],
            c_send.at[(n_kv - 1) * n_tp + i],
            c_recv.at[me],
            z,
            k,
        )
    summed = own.astype(BF16).astype(F32)
    for t, k in order[1:]:
        who = t * n_tp + k
        arrived(down_in.at[who], c_send.at[0], c_recv.at[who], t, k)
        summed += down_in[who].astype(F32)
    chip_stream = jnp.concatenate([wide_v[z * n_tp + i] for i in range(n_tp)], axis=1)
    middle = (chip_stream.astype(F32) + 0.5 * summed).astype(BF16)
    middle_v[z] = middle

    for copy in load_mix:
        copy.wait()
    middle_wide = middle.astype(F32)
    scaled = (middle_wide * mixgain_v[...]).astype(BF16)
    part = dot(scaled, proj_v[...])
    square_part = jnp.broadcast_to(
        jnp.sum(middle_wide * middle_wide, axis=1, keepdims=True), (seqs, key_cols)
    )
    queries_keys = part[:, : 2 * key_cols]
    logits_squares = jnp.concatenate([part[:, 2 * key_cols : 3 * key_cols], square_part], axis=1)
    values_part = part[:, 3 * key_cols : 3 * key_cols + value_cols]
    gates_part = part[:, 3 * key_cols + value_cols :]
    for j in range(n_kv):
        mine = slice(j * rows, (j + 1) * rows)
        proj_out[j] = jnp.concatenate(
            [queries_keys[mine], logits_squares[mine], values_part[mine], gates_part[mine]], axis=0
        )
    for j, t in enumerate(far):
        send(proj_out.at[t], proj_in.at[z], d_send.at[j], d_recv.at[z], t, c)
    for j, t in enumerate(far):
        send(middle_v.at[z], middle_v.at[z], m_send.at[j], m_recv.at[z], t, c)

    for copy in load_small:
        copy.wait()
    load_state.wait()
    load_output.wait()
    total = proj_out[z]
    for t in far[::-1]:
        arrived(proj_in.at[t], d_send.at[0], d_recv.at[t], t, c)
        total += proj_in[t]
    scale = lax.rsqrt(total[rows : 2 * rows, key_cols : key_cols + 1] / width + EPSILON)
    query = total[:rows, :key_cols] * (scale * key_dim ** (-0.5))
    keys = total[:rows, key_cols:] * scale
    logits = total[rows : 2 * rows, :key_cols] * scale
    values = total[2 * rows : 3 * rows] * scale
    outgate = total[3 * rows :] * scale
    log_sigmoid = jnp.minimum(logits, 0.0) - jnp.log(1.0 + jnp.exp(-jnp.abs(logits)))
    decay = jnp.exp(log_sigmoid / GATE_SOFTNESS - amounts_v[...])
    stacked = jnp.concatenate(
        [query, keys, decay, jnp.zeros((-3 * rows % 8, key_cols), F32)], axis=0
    )
    turned = stacked.T
    gated = headgain_v[...] * jax.nn.silu(outgate)
    readouts, gates = [], []
    for h in range(heads):
        span = slice(h * key_dim, (h + 1) * key_dim)
        lane = slice(h * value_dim, (h + 1) * value_dim)
        gates.append(gated[:, lane])
        for b in range(rows):
            q_col = turned[span, b : b + 1]
            k_col = turned[span, rows + b : rows + b + 1]
            d_col = turned[span, 2 * rows + b : 2 * rows + b + 1]
            new = d_col * state_v[b, h] + k_col * values[b : b + 1, lane]
            newstate_v[b, h] = new
            readouts.append(jnp.sum(q_col * new, axis=0, keepdims=True))
    readout = jnp.concatenate(readouts, axis=0)
    normed = readout * lax.rsqrt(jnp.mean(readout * readout, axis=1, keepdims=True) + EPSILON)

    mixed_v[z] = (normed * jnp.concatenate(gates, axis=0)).astype(BF16).astype(F32)
    for j, t in enumerate(far):
        send(mixed_v.at[z], mixed_v.at[z], e_send.at[j], e_recv.at[z], t, c)
    for t in far[::-1]:
        arrived(mixed_v.at[t], e_send.at[0], e_recv.at[t], t, c)
    blocks = [mixed_v[j] for j in range(n_kv)]
    mixed = jnp.concatenate(
        [
            jnp.concatenate([block[h * rows : (h + 1) * rows] for block in blocks], axis=0)
            for h in range(heads)
        ],
        axis=1,
    ).astype(BF16)
    attn_v[me] = dot(mixed, output_v[...]).astype(BF16)

    for p, (t, k) in enumerate(peers):
        send(attn_v.at[me], attn_v.at[me], g_send.at[p], g_recv.at[me], t, k)
    for copy in load_second:
        copy.wait()
    gate_acc = jnp.zeros((seqs, gate2_v.shape[0]), F32)
    up_acc = jnp.zeros((seqs, up2_v.shape[0]), F32)
    squares = jnp.zeros((seqs, 1), F32)
    for t in [z] + far[::-1]:
        if t is not z:
            arrived(middle_v.at[t], m_send.at[0], m_recv.at[t], t, c)
        attention = jnp.zeros((seqs, chip_cols), F32)
        for k in cores:
            who = t * n_tp + k
            if not (t is z and k is cores[0]):
                arrived(attn_v.at[who], g_send.at[0], g_recv.at[who], t, k)
            attention += attn_v[who].astype(F32)
        after = (middle_v[t].astype(F32) + attention).astype(BF16)
        block = after.astype(F32)
        if t is z:
            for i in range(n_tp):
                after_v[i] = block[:, i * own_cols : (i + 1) * own_cols]
        cols = pl.ds(pl.multiple_of(t * chip_cols, chip_cols), chip_cols)
        scaled = (block * gain2_v[:, cols]).astype(BF16)
        squares += jnp.sum(block * block, axis=1, keepdims=True)
        gate_acc += dot_t(scaled, gate2_v[:, cols])
        up_acc += dot_t(scaled, up2_v[:, cols])
    scale = lax.rsqrt(squares / width + EPSILON)
    hidden = (jax.nn.silu(gate_acc * scale) * (up_acc * scale)).astype(BF16)

    load_down2.wait()
    for j, t in enumerate(far):
        cols = pl.ds(pl.multiple_of(t * chip_cols, chip_cols), chip_cols)
        piece = dot(hidden, down2_v[:, cols]).astype(BF16)
        for k in range(n_tp):
            last_out[j, k] = piece[:, k * own_cols : (k + 1) * own_cols]
            send(last_out.at[j, k], last_in.at[me], h_send.at[j * n_tp + k], h_recv.at[me], t, k)
    cols = pl.ds(pl.multiple_of(z * chip_cols, chip_cols), chip_cols)
    piece = dot(hidden, down2_v[:, cols]).astype(BF16)
    for k in range(n_tp):
        last_out[n_kv - 1, k] = piece[:, k * own_cols : (k + 1) * own_cols]
    for i, k in enumerate(cores[1:]):
        send(
            last_out.at[n_kv - 1, k],
            last_in.at[me],
            h_send.at[(n_kv - 1) * n_tp + i],
            h_recv.at[me],
            z,
            k,
        )
    summed = last_out[n_kv - 1, c].astype(F32)
    for t, k in order[1:]:
        who = t * n_tp + k
        arrived(last_in.at[who], h_send.at[0], h_recv.at[who], t, k)
        summed += last_in[who].astype(F32)
    out_ref[...] = (after_v[c] + 0.5 * summed).astype(BF16)

    for copy in sent:
        copy.wait_send()


def store_kernel(stream_v, state_v, stream_h, state_h, sem):
    copies = [
        pltpu.make_async_copy(state_v, state_h, sem.at[0]),
        pltpu.make_async_copy(stream_v, stream_h, sem.at[1]),
    ]
    for copy in copies:
        copy.start()
    for copy in copies:
        copy.wait()


def half_block(stream, norm_gain, w_gate, w_up, w_down):
    wide = lax.all_gather(stream, ("kv", "tp"), axis=1, tiled=True).astype(jnp.float32)
    scaled = (wide * norm_gain).astype(jnp.bfloat16)
    gate_acc = jnp.dot(scaled, w_gate, preferred_element_type=jnp.float32)
    up_acc = jnp.dot(scaled, w_up, preferred_element_type=jnp.float32)
    square_acc = jnp.sum(wide * wide, axis=1)
    row_scale = lax.rsqrt(square_acc / norm_gain.shape[0] + EPSILON)[:, None]
    hidden = (jax.nn.silu(gate_acc * row_scale) * (up_acc * row_scale)).astype(jnp.bfloat16)
    partial_out = jnp.dot(hidden, w_down, preferred_element_type=jnp.float32)
    summed = lax.psum_scatter(partial_out, ("kv", "tp"), scatter_dimension=1, tiled=True)
    return (stream.astype(jnp.float32) + 0.5 * summed).astype(jnp.bfloat16)


def portable_body(
    stream,
    old_state,
    decay_amounts,
    first_gain,
    first_gate,
    first_up,
    first_down,
    mixer_gain,
    query_weight,
    key_weight,
    decay_weight,
    value_weight,
    output_gate_weight,
    head_gain,
    output_weight,
    second_gain,
    second_gate,
    second_up,
    second_down,
):
    middle = half_block(stream, first_gain, first_gate, first_up, first_down)
    paired_cols = lax.all_gather(middle, "tp", axis=1, tiled=True)
    wide_cols = paired_cols.astype(jnp.float32)
    scaled = (wide_cols * mixer_gain).astype(jnp.bfloat16)
    query_part = jnp.dot(scaled, query_weight, preferred_element_type=jnp.float32)
    key_part = jnp.dot(scaled, key_weight, preferred_element_type=jnp.float32)
    decay_part = jnp.dot(scaled, decay_weight, preferred_element_type=jnp.float32)
    value_part = jnp.dot(scaled, value_weight, preferred_element_type=jnp.float32)
    outgate_part = jnp.dot(scaled, output_gate_weight, preferred_element_type=jnp.float32)
    local_rows = old_state.shape[0]
    local_heads = old_state.shape[1]
    key_dim = old_state.shape[2]
    value_dim = old_state.shape[3]
    query_sum, key_sum, decay_sum, value_sum, outgate_sum, own_squares = (
        lax.psum_scatter(query_part, "kv", scatter_dimension=0, tiled=True),
        lax.psum_scatter(key_part, "kv", scatter_dimension=0, tiled=True),
        lax.psum_scatter(decay_part, "kv", scatter_dimension=0, tiled=True),
        lax.psum_scatter(value_part, "kv", scatter_dimension=0, tiled=True),
        lax.psum_scatter(outgate_part, "kv", scatter_dimension=0, tiled=True),
        lax.psum_scatter(
            jnp.sum(wide_cols * wide_cols, axis=1), "kv", scatter_dimension=0, tiled=True
        ),
    )
    row_scale = lax.rsqrt(own_squares / first_gain.shape[0] + EPSILON)[:, None]
    query = (query_sum * row_scale * key_dim ** (-0.5)).reshape(local_rows, local_heads, key_dim)
    keys = (key_sum * row_scale).reshape(local_rows, local_heads, key_dim)
    gate_logits = (decay_sum * row_scale).reshape(local_rows, local_heads, key_dim)
    values = (value_sum * row_scale).reshape(local_rows, local_heads, value_dim)
    decay_logarithm = jax.nn.log_sigmoid(gate_logits) / GATE_SOFTNESS - decay_amounts.reshape(
        local_rows, local_heads, key_dim
    )
    new_state = (
        jnp.exp(decay_logarithm)[..., None] * old_state + keys[..., None] * values[:, :, None, :]
    )
    readout = jnp.einsum("bhk,bhkv->bhv", query, new_state, precision=lax.Precision.HIGHEST)
    normed = readout * lax.rsqrt(jnp.mean(readout * readout, axis=-1, keepdims=True) + EPSILON)
    mixed_heads = (
        normed.reshape(local_rows, local_heads * value_dim)
        * head_gain
        * jax.nn.silu(outgate_sum * row_scale)
    ).astype(jnp.bfloat16)
    projected = jnp.dot(
        lax.all_gather(mixed_heads, "kv", axis=0, tiled=True),
        output_weight,
        preferred_element_type=jnp.float32,
    ).astype(jnp.bfloat16)
    attention_out = lax.psum_scatter(
        lax.optimization_barrier(projected).astype(jnp.float32).astype(jnp.bfloat16),
        "tp",
        scatter_dimension=1,
        tiled=True,
    ).astype(jnp.float32)
    after = (middle.astype(jnp.float32) + attention_out).astype(jnp.bfloat16)
    mixed_stream = half_block(after, second_gain, second_gate, second_up, second_down)
    return (mixed_stream, new_state)


def body(n_kv, n_tp, *args):
    (
        stream,
        old_state,
        decay_amounts,
        first_gain,
        first_gate,
        first_up,
        first_down,
        mixer_gain,
        query_weight,
        key_weight,
        decay_weight,
        value_weight,
        output_gate_weight,
        head_gain,
        output_weight,
        second_gain,
        second_gate,
        second_up,
        second_down,
    ) = args
    seqs, own_cols = stream.shape
    chip_cols = own_cols * n_tp
    rows, heads, key_dim, value_dim = old_state.shape
    if own_cols % 128 or value_dim != 2 * key_dim or value_dim % 128 or n_kv * n_tp > 16:
        return portable_body(*args)
    proj_cols = 3 * heads * key_dim + 2 * heads * value_dim
    n = n_kv * n_tp
    first_gain, mixer_gain, head_gain, second_gain = (
        g.reshape(1, -1) for g in (first_gain, mixer_gain, head_gain, second_gain)
    )

    first_gate, first_up, second_gate, second_up = (
        w.T for w in (first_gate, first_up, second_gate, second_up)
    )

    def like(array):
        return pltpu.VMEM(array.shape, array.dtype)

    dma = pltpu.SemaphoreType.DMA
    scratch = [
        like(stream),
        like(old_state),
        like(decay_amounts),
        like(first_gain),
        like(first_gate),
        like(first_up),
        like(first_down),
        like(mixer_gain),
        pltpu.VMEM((chip_cols, proj_cols), BF16),
        like(head_gain),
        like(output_weight),
        like(second_gain),
        like(second_gate),
        like(second_up),
        like(second_down),
        pltpu.VMEM((n, seqs, own_cols), BF16),
        pltpu.VMEM((n_kv, seqs, chip_cols), BF16),
        pltpu.VMEM((n, seqs, chip_cols), BF16),
        pltpu.VMEM((n_kv, seqs, chip_cols), BF16),
        pltpu.VMEM((n_kv, 4 * rows, heads * value_dim), F32),
        pltpu.VMEM((n_kv, 4 * rows, heads * value_dim), F32),
        pltpu.VMEM((n_kv, heads * rows, value_dim), F32),
        pltpu.VMEM((n, seqs, chip_cols), BF16),
        pltpu.VMEM((n_tp, seqs, own_cols), F32),
        pltpu.VMEM((n_kv, n_tp, seqs, own_cols), BF16),
        pltpu.VMEM((n, seqs, own_cols), BF16),
        dma((19,)),
        dma((n,)),
        dma((n,)),
        dma((n,)),
        dma((n,)),
        dma((n_kv,)),
        dma((n_kv,)),
        dma((n_kv,)),
        dma((n_kv,)),
        dma((n_kv,)),
        dma((n_kv,)),
        dma((n,)),
        dma((n,)),
        dma((n,)),
        dma((n,)),
    ]
    mixed_stream, new_state = pl.pallas_call(
        functools.partial(layer_kernel, n_kv, n_tp),
        out_shape=(
            pltpu.VMEM(stream.shape, stream.dtype),
            pltpu.VMEM(old_state.shape, old_state.dtype),
        ),
        in_specs=[pl.BlockSpec(memory_space=pl.ANY)] * 19,
        out_specs=(
            pl.BlockSpec(memory_space=pltpu.VMEM),
            pl.BlockSpec(memory_space=pltpu.VMEM),
        ),
        scratch_shapes=scratch,
        compiler_params=pltpu.CompilerParams(
            collective_id=0, has_side_effects=True, vmem_limit_bytes=60 * 1024 * 1024
        ),
        name="layer",
    )(
        stream,
        old_state,
        decay_amounts,
        first_gain,
        first_gate,
        first_up,
        first_down,
        mixer_gain,
        query_weight,
        key_weight,
        decay_weight,
        value_weight,
        output_gate_weight,
        head_gain,
        output_weight,
        second_gain,
        second_gate,
        second_up,
        second_down,
    )
    return pl.pallas_call(
        store_kernel,
        out_shape=(
            jax.ShapeDtypeStruct(stream.shape, stream.dtype),
            jax.ShapeDtypeStruct(old_state.shape, old_state.dtype),
        ),
        in_specs=[pl.BlockSpec(memory_space=pltpu.VMEM)] * 2,
        out_specs=(pl.BlockSpec(memory_space=pl.ANY),) * 2,
        scratch_shapes=[dma((2,))],
        name="store",
    )(
        pltpu.with_memory_space_constraint(mixed_stream, pltpu.VMEM),
        pltpu.with_memory_space_constraint(new_state, pltpu.VMEM),
    )


def solution(mesh):
    in_specs = (
        P("dp", ("kv", "tp")),
        P(("dp", "kv"), "tp", None, None),
        P(("dp", "kv"), "tp"),
        P(),
        P(None, ("kv", "tp")),
        P(None, ("kv", "tp")),
        P(("kv", "tp"), None),
        P("kv"),
        P("kv", "tp"),
        P("kv", "tp"),
        P("kv", "tp"),
        P("kv", "tp"),
        P("kv", "tp"),
        P("tp"),
        P("tp", "kv"),
        P(),
        P(None, ("kv", "tp")),
        P(None, ("kv", "tp")),
        P(("kv", "tp"), None),
    )
    out_specs = (P("dp", ("kv", "tp")), P(("dp", "kv"), "tp", None, None))
    return jax.shard_map(
        functools.partial(body, mesh.shape["kv"], mesh.shape["tp"]),
        mesh=mesh,
        in_specs=in_specs,
        out_specs=out_specs,
        check_vma=False,
    )
```
